512 devices in a mesh: grp: 2 (over y), ep: 16 (over z), tp: 16 (over x, core).
Axes of the slice: x: 8, y: 2, z: 16, core: 2. Of those that a mesh axis runs over, the one named last changes fastest.
The devices are a block of a 8x16x16 slice.
Arguments:
- tokens: bfloat16 [192, 2048], P('grp', 'ep'), parts along dimension 0, may hold values from -70 to 70
- first_gain: float32 [2048], replicated, may hold values from 0.1 to 1.9
- w_query: bfloat16 [2048, 2048], P('ep', 'tp'), may hold values from -0.125 to 0.125
- w_key: bfloat16 [2048, 2048], P('ep', 'tp'), may hold values from -0.125 to 0.125
- w_value: bfloat16 [2048, 4096], P('ep', 'tp'), may hold values from -0.125 to 0.125
- w_outgate: bfloat16 [2048, 4096], P('ep', 'tp'), may hold values from -0.125 to 0.125
- w_input: bfloat16 [2048, 16], replicated, may hold values from -0.125 to 0.125
- w_forget: bfloat16 [2048, 16], replicated, may hold values from -0.125 to 0.125
- input_bias: float32 [16], replicated, may hold values from -3 to 3
- forget_bias: float32 [16], replicated, may hold values from -2 to 5
- head_gain: float32 [4096], replicated, may hold values from 0.1 to 1.9
- w_project: bfloat16 [4096, 2048], P('tp', 'ep'), may hold values from -0.09375 to 0.09375
- cell_state: float32 [192, 16, 128, 256], P(('grp', 'ep'), 'tp'), parts along dimension 0, may hold values from -6 to 6
- norm_state: float32 [192, 16, 128], P(('grp', 'ep'), 'tp'), parts along dimension 0, may hold values from -6 to 6
- max_state: float32 [192, 16], P(('grp', 'ep'), 'tp'), parts along dimension 0, may hold values from -110 to 110
- second_gain: float32 [2048], replicated, may hold values from 0.1 to 1.9
- routes: int32 [192, 2], P('grp'), parts along dimension 0, may hold values from 0 to 15, all different within a row; in each aligned block of 6 rows (0 to 5, 6 to 11, ...) at most 2 rows name the same one
- route_weight: float32 [192, 2], P('grp'), parts along dimension 0, may hold values from 0.2 to 1
- expert_gate: bfloat16 [16, 2048, 4096], P('ep', None, 'tp'), may hold values from -0.125 to 0.125
- expert_up: bfloat16 [16, 2048, 4096], P('ep', None, 'tp'), may hold values from -0.125 to 0.125
- expert_down: bfloat16 [16, 4096, 2048], P('ep', 'tp'), may hold values from -0.09375 to 0.09375
Outputs:
- layer_out: bfloat16 [192, 2048], P('grp', 'ep'), parts along dimension 0
- new_cell: float32 [192, 16, 128, 256], P(('grp', 'ep'), 'tp'), parts along dimension 0
- new_norm: float32 [192, 16, 128], P(('grp', 'ep'), 'tp'), parts along dimension 0
- new_max: float32 [192, 16], P(('grp', 'ep'), 'tp'), parts along dimension 0
The draws below stay inside these ranges and needn't reach their ends.
There are 2 independent parts, one for each index of `grp`. The reference program is written for one: setup_inputs(seed, part) draws one part's arguments, and reference() takes and returns one part's arrays. A program takes and returns all parts, laid end to end along the dimension named above; an argument that names none is the same for every part. Nothing has to cross between parts.
Inputs may be any that keep to these rules, and one draw needn't show every extreme that they name: `routes`: each sequence names 2 different experts. In each aligned block of 6 sequences no expert is named by more than 2 of them, a bound that some block reaches.
All inputs are finite; a program needn't handle non-finite values.
Results may differ from the reference program's by a relative error of at most 0.0065.
Values may be sent and summed in bfloat16 or wider, within the bound.
No kernel may reach another device: no remote copies, remote signals or barrier semaphores. Data moves between devices by JAX's collectives and lax.ppermute only.
A program may use at most 64 MiB of HBM per device.

```python
import math
import jax
import jax.numpy as jnp
import numpy as np
from jax import lax

D = 2048
HEADS = 16
DK = 128
DV = 256
FF = 4096
TOP = 2
SEQ_DEV = 6
EXPERTS = 16
SEQS = 96
CAP = 2
N_EP = 16


def draw_tokens(key, part):
    key_base, key_cols = jax.random.split(key, 2)
    position = jnp.arange(D, dtype=jnp.float32) / D
    drawn = jnp.clip(jax.random.normal(key_base, (SEQS, D), jnp.float32), -4.0, 4.0)
    column_scale = 4.0 ** position * jax.random.uniform(key_cols, (D,), jnp.float32, 0.6, 1.2)
    values = drawn * column_scale
    return values.astype(jnp.bfloat16)


def draw_max_state(key, part):
    key_base = jax.random.fold_in(key, 0)
    drawn = jax.random.uniform(key_base, (SEQS, HEADS), jnp.float32, -3.0, 3.0)
    return drawn


def shard_levels(key, dims, shards, least, high):
    gain, own = 1.0, jax.random.fold_in(key, 6)
    for dim, blocks in shards:
        steps = jnp.exp(jax.random.uniform(jax.random.fold_in(own, dim), (blocks,), jnp.float32, least / len(shards), high / len(shards)))
        gain = gain * jnp.repeat(steps, dims[dim] // blocks).reshape([-1 if axis == dim else 1 for axis in range(len(dims))])
    return gain


def shared_out(own_key, own, number, rows, count, top, limit, skew):
    ranking = jax.random.permutation(own_key, count)
    crowded, ordinary = portions_of(count, rows * top, limit, skew, True), portions_of(count, rows * top, limit, skew, False)
    places = jnp.arange(count)

    def named(lengths, turn):
        used = int((lengths > 0).sum())
        fixed = max(1, used // 4)
        moved = fixed + (places - fixed + turn * (used - fixed)) % max(1, count - fixed)
        return jnp.zeros((count,), jnp.int32).at[ranking[jnp.where(places < fixed, places, moved)]].set(jnp.asarray(lengths, jnp.int32))

    lengths = jnp.where(number % 4 == 0, named(crowded, number // 4), named(ordinary, number - number // 4 - 1))
    mixed = jax.random.permutation(jax.random.fold_in(own, 3), count)
    donor, taker = mixed[0:count // 2 * 2:2], mixed[1:count // 2 * 2:2]
    margin = jnp.minimum(lengths[donor] - 1, limit - lengths[taker]) // 2
    margin = jnp.where((donor == ranking[0]) | (taker == ranking[0]) | (lengths[taker] == 0), 0, jnp.maximum(margin, 0))
    moved = jax.random.randint(jax.random.fold_in(own, 4), (count // 2,), 0, 1 << 20) % (margin + 1)
    lengths = lengths.at[donor].add(-moved).at[taker].add(moved)
    labels = jnp.searchsorted(jnp.cumsum(lengths), jnp.arange(rows * top), side="right").astype(jnp.int32)
    listing = labels.reshape(top, rows).T
    listing = listing[jax.random.permutation(jax.random.fold_in(own, 1), rows)]
    turn = jax.random.randint(jax.random.fold_in(own, 2), (rows, 1), 0, top)
    return jnp.take_along_axis(listing, (jnp.arange(top)[None, :] + turn) % top, axis=1)


def portions_of(number_of, total, limit, skew, full):
    loads = [(1 << 20) // math.isqrt(rank ** skew) + 1 for rank in range(1, number_of + 1)]
    largest = limit if full else min(limit, max(-(-total // number_of), total * loads[0] // sum(loads)))
    least = 1 if total - largest >= number_of - 1 else 0
    given, spare = [largest] + [least] * (number_of - 1), total - largest - least * (number_of - 1)
    while spare > 0:
        free = [i for i in range(1, number_of) if given[i] < largest] or [i for i in range(1, number_of) if given[i] < limit]
        whole, left = sum([loads[i] for i in free]), spare
        for i in free:
            extra = min(limit - given[i], max(1, left * loads[i] // whole), spare)
            given[i] = given[i] + extra
            spare = spare - extra
    return np.array(given)


def bell_draw(rng, shape, scale, reach, pieces=(), held_as=jnp.bfloat16):
    array = scale * jax.random.normal(rng, shape, jnp.float32)
    if pieces:
        array = array * shard_levels(rng, shape, pieces, -0.22, 0.18)
    return jnp.clip(array, -reach, reach).astype(held_as)


def setup_inputs(seed: int = 0, part: int = 0) -> dict:
    keys = jax.random.split(jax.random.key(seed), 22)
    part_splits = jax.random.split(jax.random.fold_in(keys[21], part), 22)
    tokens = draw_tokens(jax.random.fold_in(jax.random.fold_in(keys[21], part), 71), part)
    first_gain = jnp.clip(1.0 + 0.18 * jax.random.normal(keys[1], (D,), jnp.float32), 0.1, 1.9)
    w_query = bell_draw(keys[2], (D, HEADS * DK), D ** -0.5, 0.125, ((0, 16), (1, 16)))
    w_key = bell_draw(keys[3], (D, HEADS * DK), D ** -0.5, 0.125, ((0, 16), (1, 16)))
    w_value = bell_draw(keys[4], (D, HEADS * DV), D ** -0.5, 0.125, ((0, 16), (1, 16)))
    w_outgate = bell_draw(keys[5], (D, HEADS * DV), D ** -0.5, 0.125, ((0, 16), (1, 16)))
    w_input = bell_draw(keys[6], (D, HEADS), D ** -0.5, 0.125)
    w_forget = bell_draw(keys[7], (D, HEADS), D ** -0.5, 0.125)
    input_bias = jnp.clip(jax.random.uniform(keys[8], (HEADS,), jnp.float32, -3.0, 3.0), -3.0, 3.0)
    forget_bias = jnp.clip(jax.random.uniform(keys[9], (HEADS,), jnp.float32, -2.0, 5.0), -2.0, 5.0)
    head_gain = jnp.clip(1.0 + 0.18 * jax.random.normal(keys[10], (HEADS * DV,), jnp.float32), 0.1, 1.9)
    w_project = bell_draw(keys[11], (HEADS * DV, D), (HEADS * DV) ** -0.5, 0.09375, ((0, 16), (1, 16)))
    cell_state = bell_draw(part_splits[12], (SEQS, HEADS, DK, DV), 1.0, 6.0, ((0, 16), (1, 16)), jnp.float32)
    norm_state = bell_draw(part_splits[13], (SEQS, HEADS, DK), 1.0, 6.0, ((0, 16), (1, 16)), jnp.float32)
    max_state = draw_max_state(jax.random.fold_in(jax.random.fold_in(keys[21], part), 71), part)
    second_gain = jnp.clip(1.0 + 0.18 * jax.random.normal(keys[15], (D,), jnp.float32), 0.1, 1.9)
    routes_keys = jax.random.split(jax.random.fold_in(part_splits[16], 1), SEQS // SEQ_DEV)
    routes_turns = jax.random.permutation(jax.random.fold_in(part_splits[16], 3), SEQS // SEQ_DEV)
    routes = jax.vmap(lambda own, number: shared_out(jax.random.fold_in(part_splits[16], 2), own, number, SEQ_DEV, EXPERTS, TOP, CAP, 2))(routes_keys, routes_turns).reshape((SEQS, TOP))
    route_weight = jnp.clip(jnp.exp(jax.random.uniform(part_splits[17], (SEQS, TOP), jnp.float32, math.log(0.2), math.log(1.0))), 0.2, 1.0)
    expert_gate = bell_draw(keys[18], (EXPERTS, D, FF), D ** -0.5, 0.125, ((0, 16), (2, 16)))
    expert_up = bell_draw(keys[19], (EXPERTS, D, FF), D ** -0.5, 0.125, ((0, 16), (2, 16)))
    expert_down = bell_draw(keys[20], (EXPERTS, FF, D), FF ** -0.5, 0.09375, ((0, 16), (1, 16)))
    return dict(tokens=tokens, first_gain=first_gain, w_query=w_query, w_key=w_key, w_value=w_value, w_outgate=w_outgate, w_input=w_input, w_forget=w_forget, input_bias=input_bias, forget_bias=forget_bias, head_gain=head_gain, w_project=w_project, cell_state=cell_state, norm_state=norm_state, max_state=max_state, second_gain=second_gain, routes=routes, route_weight=route_weight, expert_gate=expert_gate, expert_up=expert_up, expert_down=expert_down)


NORM_EPS = 1e-05
HEAD_EPS = 1e-06

def layer_norm(stream_rows, gain_cols):
    values = stream_rows.astype(jnp.float32)
    row_mean = lax.optimization_barrier(jnp.mean(values, axis=1, keepdims=True))
    spread = lax.optimization_barrier(jnp.mean(values * values, axis=1, keepdims=True)) - row_mean * row_mean
    return ((values - row_mean) * lax.rsqrt(spread + NORM_EPS) * gain_cols).astype(jnp.bfloat16)

def routing_tables(routes, route_weight, blocks, capacity, experts):
    seq_total = routes.shape[0]
    seq_local = seq_total // blocks
    expert_ids = lax.broadcasted_iota(jnp.int32, (1, 1, experts), 2)
    matches = routes[:, :, None] == expert_ids
    routed = lax.optimization_barrier(jnp.sum(matches.astype(jnp.int32), axis=1))
    combine = lax.optimization_barrier(jnp.sum(jnp.where(matches, route_weight[:, :, None], 0.0), axis=1))
    running = jnp.cumsum(routed.reshape(blocks, seq_local, experts), axis=1).reshape(seq_total, experts) - routed
    block_ids = lax.broadcasted_iota(jnp.int32, (seq_total, experts), 0) // seq_local
    slot_of = block_ids * capacity + running
    slot_ids = lax.broadcasted_iota(jnp.int32, (experts, blocks * capacity, seq_total), 1)
    placed = (slot_of.T[:, None, :] == slot_ids) & (routed.T[:, None, :] > 0)
    return (placed, jnp.where(placed, combine.T[:, None, :], 0.0))

def reference(tokens, first_gain, w_query, w_key, w_value, w_outgate, w_input, w_forget, input_bias, forget_bias, head_gain, w_project, cell_state, norm_state, max_state, second_gain, routes, route_weight, expert_gate, expert_up, expert_down):
    normed = layer_norm(tokens, first_gain)
    queries = jnp.dot(normed, w_query, preferred_element_type=jnp.float32).astype(jnp.bfloat16)
    key_rows = jnp.dot(normed, w_key, preferred_element_type=jnp.float32).astype(jnp.bfloat16)
    value_rows = jnp.dot(normed, w_value, preferred_element_type=jnp.float32).astype(jnp.bfloat16)
    outgate = jnp.dot(normed, w_outgate, preferred_element_type=jnp.float32).astype(jnp.bfloat16)
    input_pre = jnp.dot(normed, w_input, preferred_element_type=jnp.float32) + input_bias
    forget_pre = jnp.dot(normed, w_forget, preferred_element_type=jnp.float32) + forget_bias
    carried = jax.nn.log_sigmoid(forget_pre) + max_state
    new_max = jnp.maximum(carried, input_pre)
    keep_old = jnp.exp(carried - new_max)
    admit_new = jnp.exp(input_pre - new_max)
    key_float = key_rows.astype(jnp.float32).reshape(SEQS, HEADS, DK)
    value_float = value_rows.astype(jnp.float32).reshape(SEQS, HEADS, DV)
    new_cell = keep_old[:, :, None, None] * cell_state + admit_new[:, :, None, None] * key_float[:, :, :, None] * value_float[:, :, None, :]
    new_norm = keep_old[:, :, None] * norm_state + admit_new[:, :, None] * key_float
    query_float = queries.astype(jnp.float32).reshape(SEQS, HEADS, DK) * DK ** (-0.5)
    readout = jnp.einsum('shk,shkv->shv', query_float, new_cell, precision=lax.Precision.HIGHEST)
    head_mean = lax.optimization_barrier(jnp.mean(readout, axis=2, keepdims=True))
    centred = readout - head_mean
    head_var = lax.optimization_barrier(jnp.mean(centred * centred, axis=2, keepdims=True))
    mixed_heads = ((centred * lax.rsqrt(head_var + HEAD_EPS)).reshape(SEQS, HEADS * DV) * head_gain * jax.nn.sigmoid(outgate.astype(jnp.float32))).astype(jnp.bfloat16)
    mixer_out = jnp.dot(mixed_heads, w_project, preferred_element_type=jnp.float32)
    stream = (tokens.astype(jnp.float32) + mixer_out).astype(jnp.bfloat16)
    second_normed = layer_norm(stream, second_gain)
    placed, weighted = routing_tables(routes, route_weight, N_EP, CAP, EXPERTS)
    picker = placed.astype(jnp.bfloat16)

    def one_expert(running_sum, packed):
        pick_rows, weight_rows, gate_w, up_w, down_w = packed
        chosen = jnp.dot(pick_rows, second_normed, preferred_element_type=jnp.float32).astype(jnp.bfloat16)
        gate_sum = jnp.dot(chosen, gate_w, preferred_element_type=jnp.float32)
        up_sum = jnp.dot(chosen, up_w, preferred_element_type=jnp.float32)
        active = (jax.nn.silu(gate_sum) * up_sum).astype(jnp.bfloat16)
        result = jnp.dot(active, down_w, preferred_element_type=jnp.float32).astype(jnp.bfloat16)
        added = jnp.dot(weight_rows.T, result.astype(jnp.float32), precision=lax.Precision.HIGHEST)
        return (running_sum + added, None)
    moe_out, unused = lax.scan(one_expert, jnp.zeros((SEQS, D), jnp.float32), (picker, weighted, expert_gate, expert_up, expert_down))
    layer_out = (stream.astype(jnp.float32) + moe_out).astype(jnp.bfloat16)
    return (layer_out, new_cell, new_norm, new_max)
```

```python
import jax
import jax.numpy as jnp
from jax import lax
from jax.sharding import PartitionSpec as P

NORM_EPS = 1e-05
HEAD_EPS = 1e-06
CAPACITY = 2


def exchanged(blocks, axis):
    return lax.all_to_all(blocks, axis, split_axis=0, concat_axis=0, tiled=True)


def from_everyone(array, axis):
    peers = lax.axis_size(axis)
    return exchanged(jnp.broadcast_to(array[None], (peers, *array.shape)), axis)


def in_pieces(values, count):
    pieces = []
    for _ in range(count - 1):
        head = lax.reduce_precision(values, 8, 7)
        pieces.append(head)
        values = values - head
    pieces.append(values)
    return pieces


def summed_over_tp(part):
    return jnp.sum(lax.all_gather(part.astype(jnp.bfloat16), "tp").astype(jnp.float32), axis=0)


def on_device(
    tokens,
    first_gain,
    w_query,
    w_key,
    w_value,
    w_outgate,
    w_input,
    w_forget,
    input_bias,
    forget_bias,
    head_gain,
    w_project,
    cell_state,
    norm_state,
    max_state,
    second_gain,
    routes,
    route_weight,
    expert_gate,
    expert_up,
    expert_down,
):
    blocks = lax.axis_size("ep")
    seq_total, columns = tokens.shape
    seq_local = seq_total // blocks
    key_size = cell_state.shape[2]
    value_size = cell_state.shape[3]
    features = columns * blocks
    col_start = lax.axis_index("ep") * columns
    head = lax.axis_index("tp")

    experts = blocks
    slot_count = blocks * CAPACITY
    expert_ids = lax.broadcasted_iota(jnp.int32, (1, 1, experts), 2)
    matches = routes[:, :, None] == expert_ids
    routed = jnp.sum(matches.astype(jnp.int32), axis=1)
    combine = jnp.sum(jnp.where(matches, route_weight[:, :, None], 0.0), axis=1)
    running = (
        jnp.cumsum(routed.reshape(blocks, seq_local, experts), axis=1).reshape(seq_total, experts)
        - routed
    )
    block_ids = lax.broadcasted_iota(jnp.int32, (seq_total, experts), 0) // seq_local
    slot_of = block_ids * CAPACITY + running
    slot_ids = lax.broadcasted_iota(jnp.int32, (experts, slot_count, seq_total), 1)
    placed = (slot_of.T[:, None, :] == slot_ids) & (routed.T[:, None, :] > 0)
    picker = placed.astype(jnp.bfloat16)
    weighted = jnp.where(placed, combine.T[:, None, :], 0.0)

    gains = lax.dynamic_slice_in_dim(first_gain, col_start, columns, 0)
    input_cols = lax.dynamic_slice(w_input, (col_start, head), (columns, 1))
    forget_cols = lax.dynamic_slice(w_forget, (col_start, head), (columns, 1))
    weights = jnp.concatenate(
        [w_query, w_key, w_value, w_outgate, input_cols, forget_cols], axis=1
    )
    gained = (weights.astype(jnp.float32) * gains[:, None]).astype(jnp.bfloat16)
    rows = jnp.concatenate([tokens, jnp.ones((1, columns), jnp.bfloat16)], axis=0)
    product = jnp.dot(rows, gained, preferred_element_type=jnp.float32)
    col_sums = product[seq_total:]
    values = tokens.astype(jnp.float32)
    block_mean = jnp.mean(values, axis=1, keepdims=True)
    offsets = values - block_mean
    moment = jnp.sum(offsets * offsets, axis=1, keepdims=True)
    centred = product[:seq_total] - block_mean * col_sums
    width = weights.shape[1] - 2

    def laid_out(part, mean_part, moment_part):
        gate = in_pieces(part[:, width:], 2)
        return jnp.concatenate(
            [part[:, :width], *gate, *in_pieces(mean_part, 3), *in_pieces(moment_part, 2)], axis=1
        )

    row_part = laid_out(centred, block_mean, moment).reshape(blocks, seq_local, -1)
    nothing = jnp.zeros((1, 1), jnp.float32)
    sum_part = laid_out(col_sums, nothing, nothing)
    outgoing = jnp.concatenate(
        [row_part, jnp.broadcast_to(sum_part[None], (blocks, 1, sum_part.shape[1]))], axis=1
    ).astype(jnp.bfloat16)
    incoming = exchanged(outgoing, "ep").astype(jnp.float32)

    means = jnp.sum(incoming[:, :seq_local, width + 4 : width + 7], axis=2, keepdims=True)
    moments = jnp.sum(incoming[:, :seq_local, width + 7 :], axis=2, keepdims=True)
    row_mean = jnp.mean(means, axis=0, keepdims=True)
    shifts = means - row_mean
    spread = jnp.sum(moments + columns * shifts * shifts, axis=0) / features
    inv_scale = lax.rsqrt(spread + NORM_EPS)
    projected = inv_scale * jnp.sum(
        incoming[:, :seq_local, : width + 4]
        + shifts * incoming[:, seq_local:, : width + 4],
        axis=0,
    )
    queries = projected[:, :key_size].astype(jnp.bfloat16)
    key_rows = projected[:, key_size : 2 * key_size].astype(jnp.bfloat16)
    value_rows = projected[:, 2 * key_size : 2 * key_size + value_size].astype(jnp.bfloat16)
    outgate = projected[:, 2 * key_size + value_size : width].astype(jnp.bfloat16)
    input_pre = (
        projected[:, width : width + 1]
        + projected[:, width + 2 : width + 3]
        + lax.dynamic_slice_in_dim(input_bias, head, 1, 0)
    )
    forget_pre = (
        projected[:, width + 1 : width + 2]
        + projected[:, width + 3 : width + 4]
        + lax.dynamic_slice_in_dim(forget_bias, head, 1, 0)
    )

    carried = jax.nn.log_sigmoid(forget_pre) + max_state
    new_max = jnp.maximum(carried, input_pre)
    keep_old = jnp.exp(carried - new_max)
    admit_new = jnp.exp(input_pre - new_max)
    key_float = key_rows.astype(jnp.float32)
    value_float = value_rows.astype(jnp.float32)
    old_cell = cell_state[:, 0]
    new_cell = (
        keep_old[:, :, None] * old_cell
        + admit_new[:, :, None] * key_float[:, :, None] * value_float[:, None, :]
    )
    new_norm = keep_old * norm_state[:, 0] + admit_new * key_float
    query_float = queries.astype(jnp.float32) * key_size ** (-0.5)
    readout = jnp.sum(query_float[:, :, None] * new_cell, axis=1)
    head_mean = jnp.mean(readout, axis=1, keepdims=True)
    around = readout - head_mean
    head_var = jnp.mean(around * around, axis=1, keepdims=True)
    gains_here = lax.dynamic_slice_in_dim(head_gain, head * value_size, value_size, 0)
    mixed_heads = (
        around
        * lax.rsqrt(head_var + HEAD_EPS)
        * gains_here
        * jax.nn.sigmoid(outgate.astype(jnp.float32))
    ).astype(jnp.bfloat16)

    all_mixed = from_everyone(mixed_heads, "ep").reshape(seq_total, value_size)
    head_terms = jnp.dot(all_mixed, w_project, preferred_element_type=jnp.float32)
    stream = (tokens.astype(jnp.float32) + summed_over_tp(head_terms)).astype(jnp.bfloat16)

    outbound = jnp.einsum(
        "eps,sd->epd", picker, stream, preferred_element_type=jnp.float32
    ).astype(jnp.bfloat16)
    arrived = lax.all_to_all(outbound, "ep", split_axis=0, concat_axis=2, tiled=True)[0]
    slot_rows = arrived.astype(jnp.float32)
    slot_mean = jnp.mean(slot_rows, axis=1, keepdims=True)
    slot_spread = jnp.mean(slot_rows * slot_rows, axis=1, keepdims=True) - slot_mean * slot_mean
    normed = (
        (slot_rows - slot_mean) * lax.rsqrt(slot_spread + NORM_EPS) * second_gain
    ).astype(jnp.bfloat16)
    gate_sum = jnp.dot(normed, expert_gate[0], preferred_element_type=jnp.float32)
    up_sum = jnp.dot(normed, expert_up[0], preferred_element_type=jnp.float32)
    active = (jax.nn.silu(gate_sum) * up_sum).astype(jnp.bfloat16)
    slot_out = jnp.dot(active, expert_down[0], preferred_element_type=jnp.float32)
    back = lax.all_to_all(
        slot_out.astype(jnp.bfloat16), "ep", split_axis=1, concat_axis=0, tiled=True
    )
    weight_table = weighted.reshape(experts * slot_count, seq_total)
    moe_part = sum(
        lax.dot_general(
            piece.astype(jnp.bfloat16),
            back,
            (((0,), (0,)), ((), ())),
            preferred_element_type=jnp.float32,
        )
        for piece in in_pieces(weight_table, 2)
    )
    layer_out = (stream.astype(jnp.float32) + summed_over_tp(moe_part)).astype(jnp.bfloat16)
    return (layer_out, new_cell[:, None], new_norm[:, None], new_max)


def solution(mesh):
    placed = (
        P("grp", "ep"),
        P(),
        P("ep", "tp"),
        P("ep", "tp"),
        P("ep", "tp"),
        P("ep", "tp"),
        P(),
        P(),
        P(),
        P(),
        P(),
        P("tp", "ep"),
        P(("grp", "ep"), "tp", None, None),
        P(("grp", "ep"), "tp", None),
        P(("grp", "ep"), "tp"),
        P(),
        P("grp", None),
        P("grp", None),
        P("ep", None, "tp"),
        P("ep", None, "tp"),
        P("ep", "tp", None),
    )
    return jax.shard_map(
        on_device,
        mesh=mesh,
        in_specs=placed,
        out_specs=(
            P("grp", "ep"),
            P(("grp", "ep"), "tp", None, None),
            P(("grp", "ep"), "tp", None),
            P(("grp", "ep"), "tp"),
        ),
        check_vma=False,
    )
```

```python
import functools

import jax
import jax.numpy as jnp
from jax import lax
from jax.experimental import pallas as pl
from jax.experimental.pallas import tpu as pltpu
from jax.sharding import PartitionSpec as P

NORM_EPS = 1e-05
HEAD_EPS = 1e-06
CAPACITY = 2
LANES = 128
PADDED = 8
GATE_SUMS = 16
F32 = jnp.float32
BF16 = jnp.bfloat16


def exchanged(blocks, axis):
    return lax.all_to_all(blocks, axis, split_axis=0, concat_axis=0, tiled=True)


def from_everyone(array, axis):
    peers = lax.axis_size(axis)
    return exchanged(jnp.broadcast_to(array[None], (peers, *array.shape)), axis)


def in_pieces(values, count):
    pieces = []
    for _ in range(count - 1):
        head = lax.reduce_precision(values, 8, 7)
        pieces.append(head)
        values = values - head
    pieces.append(values)
    return pieces


def summed_over_tp(part):
    return jnp.sum(from_everyone(part.astype(BF16), "tp").astype(F32), axis=0)


def rounded_pieces(values, count):
    pieces = []
    for _ in range(count):
        head = values.astype(BF16).astype(F32)
        pieces.append(head)
        values = values - head
    return pieces


def dot(a, b):
    return jnp.dot(a, b, preferred_element_type=F32)


def grid_index(shape):
    return lax.broadcasted_iota(jnp.int32, shape, 0), lax.broadcasted_iota(jnp.int32, shape, 1)


def one_hot(condition):
    return jnp.where(condition, 1.0, 0.0).astype(BF16)


def send_kernel(where_ref, tok_ref, gain_ref, wq, wk, wv, wo, wi, wf, out_ref, *, seq_local):
    head = where_ref[1]
    seq_total, columns = tok_ref.shape
    blocks = seq_total // seq_local
    count = blocks * PADDED
    row, col = grid_index((count, seq_total))
    spread_rows = one_hot(
        ((row & (PADDED - 1)) < seq_local)
        & (col == (row >> 3) * seq_local + (row & (PADDED - 1)))
    )
    slot = lax.broadcasted_iota(jnp.int32, (count, columns), 0) & (PADDED - 1)
    values = dot(spread_rows, tok_ref[...])
    values = jnp.where(slot == seq_local, 1.0, values)
    own = slot[:, :1] < seq_local
    block_mean = jnp.where(own, jnp.sum(values, axis=1, keepdims=True) * (1.0 / columns), 0.0)
    offsets = values - block_mean
    moment = jnp.where(own, jnp.sum(offsets * offsets, axis=1, keepdims=True), 0.0)
    gain_row = gain_ref[...]
    down, across = grid_index((columns, columns))
    gain_col = jnp.sum(jnp.where(down == across, gain_row, 0.0), axis=1, keepdims=True)
    exact = values.astype(BF16)
    parts = []
    for ref in (wq, wk, wv, wo):
        high, low = rounded_pieces(ref[...].astype(F32) * gain_col, 2)
        parts.append(dot(exact, high.astype(BF16)) + dot(exact, low.astype(BF16)))
    product = jnp.concatenate(parts, axis=1)
    tiles = product.reshape(blocks, PADDED, product.shape[1])
    sums = tiles[:, seq_local : seq_local + 1, :]
    centred = tiles - block_mean.reshape(blocks, PADDED, 1) * sums

    pick, _ = grid_index(wi.shape)

    def gate_part(ref):
        chosen = jnp.sum(jnp.where(pick == head, ref[...].astype(F32), 0.0), axis=0, keepdims=True)
        return jnp.sum(offsets * (chosen * gain_row), axis=1, keepdims=True)

    gates = [*rounded_pieces(gate_part(wi), 2), *rounded_pieces(gate_part(wf), 2)]
    lane = lax.broadcasted_iota(jnp.int32, (count, LANES), 1)
    start = jnp.where(slot[:, :1] == seq_local, GATE_SUMS, 0)
    table = jnp.zeros((count, LANES), F32)
    for k, piece in enumerate(gates):
        table = jnp.where(lane == start + k, piece, table)
    table = jnp.where(slot == PADDED - 1, 0.0, table)
    for k, piece in enumerate([*rounded_pieces(block_mean, 3), *rounded_pieces(moment, 2)]):
        table = jnp.where((lane == 4 + k) & own, piece, table)
    exact_table = table.astype(BF16)
    down, across = grid_index((count, count))
    same = (down >> 3) == (across >> 3)
    last = (down & (PADDED - 1)) == PADDED - 1
    inner = across & (PADDED - 1)
    laid = []
    for r in range(seq_local):
        laid.append(dot(one_hot(same & last & ((inner == r) | (inner == seq_local))), exact_table))
    side = jnp.concatenate(laid, axis=1).reshape(tiles.shape)
    out_ref[...] = (centred + side).astype(BF16)


def receive_kernel(
    where_ref, in_bias, for_bias, got_ref, cell_ref, norm_ref, max_ref, gain_ref,
    mixed_ref, keep_ref, admit_ref, value_ref, norm_out, max_out, *, columns
):
    head = where_ref[1]
    blocks, padded, width = got_ref.shape
    seq_local, _, key_size, value_size = cell_ref.shape
    count = blocks * padded
    got = got_ref[...].astype(F32)
    flat = got.reshape(count, width).astype(BF16)
    down, across = grid_index((count, count))
    same = (down >> 3) == (across >> 3)
    inner = across & (PADDED - 1)
    outer = down & (PADDED - 1)
    table = jnp.zeros((count, LANES), F32)
    for r in range(seq_local):
        back = one_hot(same & (outer == r) & (inner == PADDED - 1))
        table = table + dot(back, flat[:, r * LANES : (r + 1) * LANES])
    sums = dot(one_hot(same & (inner == seq_local)), flat).reshape(blocks, padded, width)
    lane = lax.broadcasted_iota(jnp.int32, (count, LANES), 1)

    def lanes(first, number):
        kept = jnp.where((lane >= first) & (lane < first + number), table, 0.0)
        return jnp.sum(kept, axis=1, keepdims=True).reshape(blocks, padded, 1)

    means = lanes(4, 3)
    row_mean = jnp.sum(means, axis=0, keepdims=True) * (1.0 / blocks)
    shifts = means - row_mean
    spread = jnp.sum(lanes(7, 2) + columns * shifts * shifts, axis=0) * (1.0 / (blocks * columns))
    inv_scale = lax.rsqrt(spread + NORM_EPS)
    projected = inv_scale * jnp.sum(got + shifts * sums, axis=0)

    def rounded(a, b):
        return projected[:, a:b].astype(BF16).astype(F32)

    query = rounded(0, key_size) * key_size**-0.5
    key = rounded(key_size, 2 * key_size)
    value = rounded(2 * key_size, 2 * key_size + value_size)
    outgate = rounded(2 * key_size + value_size, width)
    input_pre = (
        inv_scale * jnp.sum(lanes(0, 2) + shifts * lanes(GATE_SUMS, 2), axis=0) + in_bias[head]
    )[:seq_local]
    forget_pre = (
        inv_scale * jnp.sum(lanes(2, 2) + shifts * lanes(GATE_SUMS + 2, 2), axis=0)
        + for_bias[head]
    )[:seq_local]
    log_forget = jnp.minimum(forget_pre, 0.0) - jnp.log1p(jnp.exp(-jnp.abs(forget_pre)))
    carried = log_forget + max_ref[...]
    new_max = jnp.maximum(carried, input_pre)
    keep_old = jnp.exp(carried - new_max)
    admit_key = jnp.exp(input_pre - new_max) * key[:seq_local]
    max_out[...] = new_max
    keep_ref[...] = keep_old
    admit_ref[...] = admit_key
    value_ref[...] = value[:seq_local]
    norm_out[...] = keep_old * norm_ref[...] + admit_key
    turned = query.T
    rows = lax.broadcasted_iota(jnp.int32, (padded, value_size), 0)
    against_cell = jnp.zeros((padded, value_size), F32)
    for s in range(seq_local):
        one = jnp.sum(turned[:, s : s + 1] * cell_ref[s, 0], axis=0, keepdims=True)
        against_cell = jnp.where(rows == s, one, against_cell)
    scores = jnp.sum(query[:seq_local] * admit_key, axis=1, keepdims=True)
    readout = keep_old * against_cell[:seq_local] + scores * value[:seq_local]
    head_mean = jnp.mean(readout, axis=1, keepdims=True)
    around = readout - head_mean
    head_var = jnp.mean(around * around, axis=1, keepdims=True)
    gain = gain_ref[:, pl.ds(pl.multiple_of(head * value_size, LANES), value_size)]
    opened = 1.0 / (1.0 + jnp.exp(-outgate[:seq_local]))
    mixed = around * lax.rsqrt(head_var + HEAD_EPS) * gain * opened
    mixed = jnp.concatenate([mixed, jnp.zeros((padded - seq_local, value_size), F32)], axis=0)
    mixed_ref[...] = jnp.broadcast_to(mixed[None], (blocks, padded, value_size)).astype(BF16)


def in_vmem(array):
    return pltpu.with_memory_space_constraint(array, pltpu.VMEM)


def whole(shape):
    return pl.BlockSpec(shape, lambda i, where, n=len(shape): (0,) * n)


def parts_to_send(where, tokens, gain, w_query, w_key, w_value, w_outgate, w_input, w_forget, blocks):
    seq_total, columns = tokens.shape
    width = 2 * (w_query.shape[1] + w_value.shape[1])
    gate_block = pl.BlockSpec((w_input.shape[0], columns), lambda i, where: (0, where[0]))
    return pl.pallas_call(
        functools.partial(send_kernel, seq_local=seq_total // blocks),
        grid_spec=pltpu.PrefetchScalarGridSpec(
            num_scalar_prefetch=1,
            grid=(1,),
            in_specs=[
                whole(tokens.shape),
                pl.BlockSpec((1, columns), lambda i, where: (0, where[0])),
                *(whole(w.shape) for w in (w_query, w_key, w_value, w_outgate)),
                gate_block,
                gate_block,
            ],
            out_specs=whole((blocks, PADDED, width)),
        ),
        out_shape=jax.ShapeDtypeStruct((blocks, PADDED, width), BF16),
        name="send_parts",
    )(where, tokens, gain, w_query, w_key, w_value, w_outgate, w_input, w_forget)


def cell_step(where, input_bias, forget_bias, got, cell, norm, top, gain, columns):
    blocks = got.shape[0]
    seq_local, _, key_size, value_size = cell.shape
    shapes = [
        pltpu.VMEM((blocks, PADDED, value_size), BF16),
        pltpu.VMEM((seq_local, 1), F32),
        pltpu.VMEM((seq_local, key_size), F32),
        pltpu.VMEM((seq_local, value_size), F32),
        pltpu.VMEM((seq_local, key_size), F32),
        pltpu.VMEM((seq_local, 1), F32),
    ]
    scalars = pl.BlockSpec(memory_space=pltpu.SMEM)
    near = pl.BlockSpec(memory_space=pltpu.VMEM)
    return pl.pallas_call(
        functools.partial(receive_kernel, columns=columns),
        in_specs=[scalars, scalars, scalars, near, near, near, near, near],
        out_specs=[near] * len(shapes),
        out_shape=shapes,
        name="cell_step",
    )(where, input_bias, forget_bias, *(in_vmem(a) for a in (got, cell, norm, top, gain)))


def on_device(
    tokens,
    first_gain,
    w_query,
    w_key,
    w_value,
    w_outgate,
    w_input,
    w_forget,
    input_bias,
    forget_bias,
    head_gain,
    w_project,
    cell_state,
    norm_state,
    max_state,
    second_gain,
    routes,
    route_weight,
    expert_gate,
    expert_up,
    expert_down,
):
    blocks = lax.axis_size("ep")
    seq_total, columns = tokens.shape
    seq_local = seq_total // blocks
    value_size = cell_state.shape[3]
    where = jnp.stack([lax.axis_index("ep"), lax.axis_index("tp")]).astype(jnp.int32)

    experts = blocks
    slot_count = blocks * CAPACITY
    expert_ids = lax.broadcasted_iota(jnp.int32, (1, 1, experts), 2)
    matches = routes[:, :, None] == expert_ids
    routed = jnp.sum(matches.astype(jnp.int32), axis=1)
    combine = jnp.sum(jnp.where(matches, route_weight[:, :, None], 0.0), axis=1)
    running = (
        jnp.cumsum(routed.reshape(blocks, seq_local, experts), axis=1).reshape(seq_total, experts)
        - routed
    )
    block_ids = lax.broadcasted_iota(jnp.int32, (seq_total, experts), 0) // seq_local
    slot_of = block_ids * CAPACITY + running
    slot_ids = lax.broadcasted_iota(jnp.int32, (experts, slot_count, seq_total), 1)
    placed = (slot_of.T[:, None, :] == slot_ids) & (routed.T[:, None, :] > 0)
    picker = placed.astype(jnp.bfloat16)
    weighted = jnp.where(placed, combine.T[:, None, :], 0.0)

    outgoing = parts_to_send(
        where,
        tokens,
        first_gain.reshape(1, -1),
        w_query,
        w_key,
        w_value,
        w_outgate,
        w_input.T,
        w_forget.T,
        blocks,
    )
    incoming = exchanged(outgoing, "ep")
    mixed, keep_old, admit_key, value, new_norm, new_max = cell_step(
        where,
        input_bias,
        forget_bias,
        incoming,
        cell_state,
        norm_state[:, 0],
        max_state,
        head_gain.reshape(1, -1),
        columns,
    )
    new_cell = (
        keep_old[:, :, None] * cell_state[:, 0] + admit_key[:, :, None] * value[:, None, :]
    )

    all_mixed = exchanged(mixed, "ep")[:, :seq_local].reshape(seq_total, value_size)
    head_terms = jnp.dot(all_mixed, w_project, preferred_element_type=jnp.float32)
    stream = (tokens.astype(jnp.float32) + summed_over_tp(head_terms)).astype(jnp.bfloat16)

    outbound = jnp.einsum(
        "eps,sd->epd", picker, stream, preferred_element_type=jnp.float32
    ).astype(jnp.bfloat16)
    arrived = lax.all_to_all(outbound, "ep", split_axis=0, concat_axis=2, tiled=True)[0]
    slot_rows = arrived.astype(jnp.float32)
    slot_mean = jnp.mean(slot_rows, axis=1, keepdims=True)
    slot_spread = jnp.mean(slot_rows * slot_rows, axis=1, keepdims=True) - slot_mean * slot_mean
    normed = (
        (slot_rows - slot_mean) * lax.rsqrt(slot_spread + NORM_EPS) * second_gain
    ).astype(jnp.bfloat16)
    gate_sum = jnp.dot(normed, expert_gate[0], preferred_element_type=jnp.float32)
    up_sum = jnp.dot(normed, expert_up[0], preferred_element_type=jnp.float32)
    active = (jax.nn.silu(gate_sum) * up_sum).astype(jnp.bfloat16)
    slot_out = jnp.dot(active, expert_down[0], preferred_element_type=jnp.float32)
    back = exchanged(
        jnp.swapaxes(slot_out.astype(BF16).reshape(slot_count, blocks, columns), 0, 1), "ep"
    ).reshape(experts * slot_count, columns)
    weight_table = weighted.reshape(experts * slot_count, seq_total)
    moe_part = sum(
        lax.dot_general(
            piece.astype(jnp.bfloat16),
            back,
            (((0,), (0,)), ((), ())),
            preferred_element_type=jnp.float32,
        )
        for piece in in_pieces(weight_table, 2)
    )
    layer_out = (stream.astype(jnp.float32) + summed_over_tp(moe_part)).astype(jnp.bfloat16)
    return (layer_out, new_cell[:, None], new_norm[:, None], new_max)


def solution(mesh):
    placed = (
        P("grp", "ep"),
        P(),
        P("ep", "tp"),
        P("ep", "tp"),
        P("ep", "tp"),
        P("ep", "tp"),
        P(),
        P(),
        P(),
        P(),
        P(),
        P("tp", "ep"),
        P(("grp", "ep"), "tp", None, None),
        P(("grp", "ep"), "tp", None),
        P(("grp", "ep"), "tp"),
        P(),
        P("grp", None),
        P("grp", None),
        P("ep", None, "tp"),
        P("ep", None, "tp"),
        P("ep", "tp", None),
    )
    return jax.shard_map(
        on_device,
        mesh=mesh,
        in_specs=placed,
        out_specs=(
            P("grp", "ep"),
            P(("grp", "ep"), "tp", None, None),
            P(("grp", "ep"), "tp", None),
            P(("grp", "ep"), "tp"),
        ),
        check_vma=False,
    )
```

```python
import functools

import jax
import jax.numpy as jnp
from jax import lax
from jax.experimental import pallas as pl
from jax.experimental.pallas import tpu as pltpu
from jax.sharding import PartitionSpec as P

NORM_EPS = 1e-05
HEAD_EPS = 1e-06
CAPACITY = 2
LANES = 128
PADDED = 8
GATE_SUMS = 16
F32 = jnp.float32
BF16 = jnp.bfloat16


def exchanged(blocks, axis):
    return lax.all_to_all(blocks, axis, split_axis=0, concat_axis=0, tiled=True)


def in_pieces(values, count):
    pieces = []
    for _ in range(count - 1):
        head = lax.reduce_precision(values, 8, 7)
        pieces.append(head)
        values = values - head
    pieces.append(values)
    return pieces


def rounded_pieces(values, count):
    pieces = []
    for _ in range(count):
        head = values.astype(BF16).astype(F32)
        pieces.append(head)
        values = values - head
    return pieces


def dot(a, b):
    return jnp.dot(a, b, preferred_element_type=F32)


def grid_index(shape):
    return lax.broadcasted_iota(jnp.int32, shape, 0), lax.broadcasted_iota(jnp.int32, shape, 1)


def one_hot(condition):
    return jnp.where(condition, 1.0, 0.0).astype(BF16)


def send_kernel(
    tok_ref, gain_ref, wq, wk, wv, wo, wi, wf, max_ref, out_ref, max_out, *, seq_local
):
    max_out[...] = max_ref[...]
    head = lax.axis_index("tp")
    seq_total, columns = tok_ref.shape
    ours = pl.ds(pl.multiple_of(lax.axis_index("ep") * columns, LANES), columns)
    blocks = seq_total // seq_local
    count = blocks * PADDED
    row, col = grid_index((count, seq_total))
    spread_rows = one_hot(
        ((row & (PADDED - 1)) < seq_local)
        & (col == (row >> 3) * seq_local + (row & (PADDED - 1)))
    )
    slot = lax.broadcasted_iota(jnp.int32, (count, columns), 0) & (PADDED - 1)
    values = dot(spread_rows, tok_ref[...])
    values = jnp.where(slot == seq_local, 1.0, values)
    own = slot[:, :1] < seq_local
    block_mean = jnp.where(own, jnp.sum(values, axis=1, keepdims=True) * (1.0 / columns), 0.0)
    offsets = values - block_mean
    moment = jnp.where(own, jnp.sum(offsets * offsets, axis=1, keepdims=True), 0.0)
    gain_row = gain_ref[:, ours]
    down, across = grid_index((columns, columns))
    gain_col = jnp.sum(jnp.where(down == across, gain_row, 0.0), axis=1, keepdims=True)
    exact = values.astype(BF16)
    parts = []
    for ref in (wq, wk, wv, wo):
        high, low = rounded_pieces(ref[...].astype(F32) * gain_col, 2)
        parts.append(dot(exact, high.astype(BF16)) + dot(exact, low.astype(BF16)))
    product = jnp.concatenate(parts, axis=1)
    tiles = product.reshape(blocks, PADDED, product.shape[1])
    sums = tiles[:, seq_local : seq_local + 1, :]
    centred = tiles - block_mean.reshape(blocks, PADDED, 1) * sums

    pick, _ = grid_index((wi.shape[0], columns))

    def gate_part(ref):
        chosen = jnp.sum(jnp.where(pick == head, ref[:, ours].astype(F32), 0.0), axis=0, keepdims=True)
        return jnp.sum(offsets * (chosen * gain_row), axis=1, keepdims=True)

    gates = [*rounded_pieces(gate_part(wi), 2), *rounded_pieces(gate_part(wf), 2)]
    lane = lax.broadcasted_iota(jnp.int32, (count, LANES), 1)
    start = jnp.where(slot[:, :1] == seq_local, GATE_SUMS, 0)
    table = jnp.zeros((count, LANES), F32)
    for k, piece in enumerate(gates):
        table = jnp.where(lane == start + k, piece, table)
    table = jnp.where(slot == PADDED - 1, 0.0, table)
    for k, piece in enumerate([*rounded_pieces(block_mean, 3), *rounded_pieces(moment, 2)]):
        table = jnp.where((lane == 4 + k) & own, piece, table)
    exact_table = table.astype(BF16)
    down, across = grid_index((count, count))
    same = (down >> 3) == (across >> 3)
    last = (down & (PADDED - 1)) == PADDED - 1
    inner = across & (PADDED - 1)
    laid = []
    for r in range(seq_local):
        laid.append(dot(one_hot(same & last & ((inner == r) | (inner == seq_local))), exact_table))
    side = jnp.concatenate(laid, axis=1).reshape(tiles.shape)
    out_ref[...] = (centred + side).astype(BF16)


def receive_kernel(
    in_bias, for_bias, got_ref, cell_ref, norm_ref, max_ref, gain_ref,
    mixed_ref, keep_ref, admit_ref, value_ref, norm_out, max_out, *, columns
):
    head = lax.axis_index("tp")
    blocks, padded, width = got_ref.shape
    seq_local, _, key_size, value_size = cell_ref.shape
    count = blocks * padded
    got = got_ref[...].astype(F32)
    flat = got.reshape(count, width).astype(BF16)
    down, across = grid_index((count, count))
    same = (down >> 3) == (across >> 3)
    inner = across & (PADDED - 1)
    outer = down & (PADDED - 1)
    table = jnp.zeros((count, LANES), F32)
    for r in range(seq_local):
        back = one_hot(same & (outer == r) & (inner == PADDED - 1))
        table = table + dot(back, flat[:, r * LANES : (r + 1) * LANES])
    sums = dot(one_hot(same & (inner == seq_local)), flat).reshape(blocks, padded, width)
    lane = lax.broadcasted_iota(jnp.int32, (count, LANES), 1)

    def lanes(first, number):
        kept = jnp.where((lane >= first) & (lane < first + number), table, 0.0)
        return jnp.sum(kept, axis=1, keepdims=True).reshape(blocks, padded, 1)

    means = lanes(4, 3)
    row_mean = jnp.sum(means, axis=0, keepdims=True) * (1.0 / blocks)
    shifts = means - row_mean
    spread = jnp.sum(lanes(7, 2) + columns * shifts * shifts, axis=0) * (1.0 / (blocks * columns))
    inv_scale = lax.rsqrt(spread + NORM_EPS)
    projected = inv_scale * jnp.sum(got + shifts * sums, axis=0)

    def rounded(a, b):
        return projected[:, a:b].astype(BF16).astype(F32)

    query = rounded(0, key_size) * key_size**-0.5
    key = rounded(key_size, 2 * key_size)
    value = rounded(2 * key_size, 2 * key_size + value_size)
    outgate = rounded(2 * key_size + value_size, width)
    input_pre = (
        inv_scale * jnp.sum(lanes(0, 2) + shifts * lanes(GATE_SUMS, 2), axis=0) + in_bias[head]
    )
    forget_pre = (
        inv_scale * jnp.sum(lanes(2, 2) + shifts * lanes(GATE_SUMS + 2, 2), axis=0)
        + for_bias[head]
    )
    down, across = grid_index((padded, seq_local))
    old_max = jnp.sum(jnp.where(down == across, max_ref[...], 0.0), axis=1, keepdims=True)
    log_forget = jnp.minimum(forget_pre, 0.0) - jnp.log1p(jnp.exp(-jnp.abs(forget_pre)))
    carried = log_forget + old_max
    new_max = jnp.maximum(carried, input_pre)
    keep_old = jnp.exp(carried - new_max)
    admit_key = jnp.exp(input_pre - new_max) * key
    max_out[...] = new_max[:seq_local]
    keep_ref[...] = keep_old[:seq_local]
    admit_ref[...] = admit_key[:seq_local]
    value_ref[...] = value[:seq_local]
    query_cols = query.T
    rows = lax.broadcasted_iota(jnp.int32, (padded, value_size), 0)
    against_cell = jnp.zeros((padded, value_size), F32)
    for s in range(seq_local):
        norm_out[s : s + 1] = keep_old[s : s + 1] * norm_ref[s] + admit_key[s : s + 1]
        read = jnp.sum(query_cols[:, s : s + 1] * cell_ref[s, 0], axis=0, keepdims=True)
        against_cell = jnp.where(rows == s, read, against_cell)
    scores = jnp.sum(query * admit_key, axis=1, keepdims=True)
    readout = jnp.where(rows < seq_local, keep_old * against_cell + scores * value, 0.0)
    outgate = jnp.where(rows < seq_local, outgate, 0.0)
    head_mean = jnp.mean(readout, axis=1, keepdims=True)
    around = readout - head_mean
    head_var = jnp.mean(around * around, axis=1, keepdims=True)
    gain = gain_ref[:, pl.ds(pl.multiple_of(head * value_size, LANES), value_size)]
    opened = 1.0 / (1.0 + jnp.exp(-outgate))
    mixed = around * lax.rsqrt(head_var + HEAD_EPS) * gain * opened
    mixed_ref[...] = jnp.broadcast_to(mixed[None], (blocks, padded, value_size)).astype(BF16)


def project_kernel(got_ref, weight_ref, out_ref, *, seq_local):
    blocks, padded, width = got_ref.shape
    seq_total = out_ref.shape[1]
    rows = got_ref[...].astype(F32).reshape(blocks * padded, width).astype(BF16)
    terms = dot(rows, weight_ref[...]).astype(BF16)
    row, col = grid_index((seq_total, blocks * padded))
    inner = col & (PADDED - 1)
    packed = dot(one_hot((inner < seq_local) & (row == (col >> 3) * seq_local + inner)), terms)
    out_ref[...] = jnp.broadcast_to(packed.astype(BF16)[None], out_ref.shape)


def stream_kernel(got_ref, tok_ref, picker_ref, stream_ref, out_ref):
    mixer_out = jnp.sum(got_ref[...].astype(F32), axis=0)
    stream = (tok_ref[...].astype(F32) + mixer_out).astype(BF16)
    stream_ref[...] = stream
    chosen = lax.dot_general(
        picker_ref[...], stream, (((0,), (0,)), ((), ())), preferred_element_type=F32
    )
    out_ref[...] = chosen.astype(BF16).reshape(out_ref.shape)


def expert_kernel(
    up_hbm, down_hbm, got_ref, gain_ref, gate_ref, out_ref, up_ref, down_ref, arrived
):
    fetches = [
        pltpu.make_async_copy(up_hbm, up_ref, arrived.at[0]),
        pltpu.make_async_copy(down_hbm, down_ref, arrived.at[1]),
    ]
    for fetch in fetches:
        fetch.start()
    blocks, _, columns = got_ref.shape
    values = jnp.concatenate([got_ref[e].astype(F32) for e in range(blocks)], axis=1)
    row_mean = jnp.mean(values, axis=1, keepdims=True)
    spread = jnp.mean(values * values, axis=1, keepdims=True) - row_mean * row_mean
    normed = ((values - row_mean) * lax.rsqrt(spread + NORM_EPS) * gain_ref[...]).astype(BF16)
    gate = dot(normed, gate_ref[0])
    fetches[0].wait()
    active = (gate / (1.0 + jnp.exp(-gate)) * dot(normed, up_ref[0])).astype(BF16)
    fetches[1].wait()
    result = dot(active, down_ref[0]).astype(BF16)
    for e in range(blocks):
        out_ref[e] = result[:, e * columns : (e + 1) * columns]


def combine_kernel(table_ref, back_ref, out_ref):
    seq_total = out_ref.shape[1]
    experts, slots, columns = back_ref.shape
    both = dot(table_ref[...], back_ref[...].reshape(experts * slots, columns))
    added = (both[:seq_total] + both[seq_total:]).astype(BF16)
    out_ref[...] = jnp.broadcast_to(added[None], out_ref.shape)


def in_vmem(array):
    return pltpu.with_memory_space_constraint(array, pltpu.VMEM)


def kernel_call(kernel, name, shapes, near, scalars=(), far=(), left=(), scratch=()):
    vmem = pl.BlockSpec(memory_space=pltpu.VMEM)
    smem = pl.BlockSpec(memory_space=pltpu.SMEM)
    return pl.pallas_call(
        kernel,
        in_specs=[smem] * len(scalars)
        + [pl.BlockSpec(memory_space=pl.ANY)] * len(left)
        + [vmem] * (len(far) + len(near)),
        out_specs=jax.tree.map(lambda _: vmem, shapes),
        out_shape=shapes,
        scratch_shapes=scratch,
        name=name,
    )(*scalars, *left, *far, *(in_vmem(a) for a in near))


def on_device(
    tokens,
    first_gain,
    w_query,
    w_key,
    w_value,
    w_outgate,
    w_input,
    w_forget,
    input_bias,
    forget_bias,
    head_gain,
    w_project,
    cell_state,
    norm_state,
    max_state,
    second_gain,
    routes,
    route_weight,
    expert_gate,
    expert_up,
    expert_down,
):
    blocks = lax.axis_size("ep")
    seq_total, columns = tokens.shape
    seq_local = seq_total // blocks
    value_size = cell_state.shape[3]
    experts = blocks
    slot_count = blocks * CAPACITY
    expert_ids = lax.broadcasted_iota(jnp.int32, (1, 1, experts), 2)
    matches = routes[:, :, None] == expert_ids
    routed = jnp.sum(matches.astype(jnp.int32), axis=1)
    combine = jnp.sum(jnp.where(matches, route_weight[:, :, None], 0.0), axis=1)
    running = (
        jnp.cumsum(routed.reshape(blocks, seq_local, experts), axis=1).reshape(seq_total, experts)
        - routed
    )
    block_ids = lax.broadcasted_iota(jnp.int32, (seq_total, experts), 0) // seq_local
    slot_of = block_ids * CAPACITY + running
    slot_ids = lax.broadcasted_iota(jnp.int32, (experts, slot_count, seq_total), 1)
    placed = (slot_of.T[:, None, :] == slot_ids) & (routed.T[:, None, :] > 0)
    picker = placed.astype(BF16).reshape(experts * slot_count, seq_total).T
    weighted = jnp.where(placed, combine.T[:, None, :], 0.0)

    width = 2 * (w_query.shape[1] + w_value.shape[1])
    outgoing, old_max = kernel_call(
        functools.partial(send_kernel, seq_local=seq_local),
        "send_parts",
        [pltpu.VMEM((blocks, PADDED, width), BF16), pltpu.VMEM((1, seq_local), F32)],
        (),
        far=(
            tokens,
            first_gain.reshape(1, -1),
            w_query,
            w_key,
            w_value,
            w_outgate,
            w_input.T,
            w_forget.T,
            max_state.T,
        ),
    )
    weight_rows = weighted.reshape(experts * slot_count, seq_total).T
    table = jnp.concatenate([t.astype(BF16) for t in in_pieces(weight_rows, 2)], axis=0)
    incoming, picker, table = lax.optimization_barrier((exchanged(outgoing, "ep"), picker, table))

    key_size = cell_state.shape[2]
    mixed, *updates = kernel_call(
        functools.partial(receive_kernel, columns=columns),
        "cell_step",
        [
            pltpu.VMEM((blocks, PADDED, value_size), BF16),
            pltpu.VMEM((seq_local, 1), F32),
            pltpu.VMEM((seq_local, key_size), F32),
            pltpu.VMEM((seq_local, value_size), F32),
            pltpu.VMEM((seq_local, key_size), F32),
            pltpu.VMEM((seq_local, 1), F32),
        ],
        (incoming, cell_state, norm_state, old_max, head_gain.reshape(1, -1)),
        scalars=(input_bias, forget_bias),
    )

    part_shape = pltpu.VMEM((lax.axis_size("tp"), seq_total, columns), BF16)
    head_terms = kernel_call(
        functools.partial(project_kernel, seq_local=seq_local),
        "project_heads",
        part_shape,
        (exchanged(mixed, "ep"), w_project),
    )
    stream, outbound = kernel_call(
        stream_kernel,
        "stream_rows",
        [
            pltpu.VMEM(tokens.shape, BF16),
            pltpu.VMEM((experts, slot_count, columns), BF16),
        ],
        (exchanged(head_terms, "tp"), tokens, picker),
    )

    slot_out = kernel_call(
        expert_kernel,
        "expert",
        pltpu.VMEM((blocks, slot_count, columns), BF16),
        (
            exchanged(outbound, "ep"),
            second_gain.reshape(1, -1),
            expert_gate,
        ),
        left=(expert_up, expert_down),
        scratch=(
            pltpu.VMEM(expert_up.shape, BF16),
            pltpu.VMEM(expert_down.shape, BF16),
            pltpu.SemaphoreType.DMA((2,)),
        ),
    )
    moe_terms = kernel_call(
        combine_kernel, "combine", part_shape, (table, exchanged(slot_out, "ep"))
    )
    moe_terms, *updates = lax.optimization_barrier((moe_terms, *updates))
    keep_old, admit_key, value, new_norm, new_max = updates
    new_cell = (
        keep_old[:, :, None] * cell_state[:, 0] + admit_key[:, :, None] * value[:, None, :]
    )
    moe_out = jnp.sum(exchanged(moe_terms, "tp").astype(F32), axis=0)
    layer_out = (stream.astype(F32) + moe_out).astype(BF16)
    return (layer_out, new_cell[:, None], new_norm[:, None], new_max)


def solution(mesh):
    placed = (
        P("grp", "ep"),
        P(),
        P("ep", "tp"),
        P("ep", "tp"),
        P("ep", "tp"),
        P("ep", "tp"),
        P(),
        P(),
        P(),
        P(),
        P(),
        P("tp", "ep"),
        P(("grp", "ep"), "tp", None, None),
        P(("grp", "ep"), "tp", None),
        P(("grp", "ep"), "tp"),
        P(),
        P("grp", None),
        P("grp", None),
        P("ep", None, "tp"),
        P("ep", None, "tp"),
        P("ep", "tp", None),
    )
    return jax.shard_map(
        on_device,
        mesh=mesh,
        in_specs=placed,
        out_specs=(
            P("grp", "ep"),
            P(("grp", "ep"), "tp", None, None),
            P(("grp", "ep"), "tp", None),
            P(("grp", "ep"), "tp"),
        ),
        check_vma=False,
    )
```

```python
import functools

import jax
import jax.numpy as jnp
from jax import lax
from jax.experimental import pallas as pl
from jax.experimental.pallas import tpu as pltpu
from jax.sharding import PartitionSpec as P

NORM_EPS = 1e-05
HEAD_EPS = 1e-06
CAPACITY = 2
LANES = 128
PADDED = 8
GATE_SUMS = 16
F32 = jnp.float32
BF16 = jnp.bfloat16


def exchanged(blocks, axis):
    return lax.all_to_all(blocks, axis, split_axis=0, concat_axis=0, tiled=True)


def cores_of_chips(axis):
    size = lax.axis_size(axis)
    return [[i, i + 1] for i in range(0, size, 2)]


def chips_of_cores(axis):
    size = lax.axis_size(axis)
    return [list(range(core, size, 2)) for core in range(2)]


def swapped(blocks, groups):
    return lax.all_to_all(
        blocks, "tp", split_axis=0, concat_axis=0, tiled=True, axis_index_groups=groups
    )


def in_pieces(values, count):
    pieces = []
    for _ in range(count - 1):
        head = lax.reduce_precision(values, 8, 7)
        pieces.append(head)
        values = values - head
    pieces.append(values)
    return pieces


def rounded_pieces(values, count):
    pieces = []
    for _ in range(count):
        head = values.astype(BF16).astype(F32)
        pieces.append(head)
        values = values - head
    return pieces


def dot(a, b):
    return jnp.dot(a, b, preferred_element_type=F32)


def grid_index(shape):
    return lax.broadcasted_iota(jnp.int32, shape, 0), lax.broadcasted_iota(jnp.int32, shape, 1)


def one_hot(condition):
    return jnp.where(condition, 1.0, 0.0).astype(BF16)


def send_kernel(
    tok_ref, gain_ref, wq, wk, wv, wo, wi, wf, max_ref, out_ref, max_out, *, seq_local
):
    max_out[...] = max_ref[...]
    head = lax.axis_index("tp")
    seq_total, columns = tok_ref.shape
    ours = pl.ds(pl.multiple_of(lax.axis_index("ep") * columns, LANES), columns)
    blocks = seq_total // seq_local
    count = blocks * PADDED
    row, col = grid_index((count, seq_total))
    spread_rows = one_hot(
        ((row & (PADDED - 1)) < seq_local)
        & (col == (row >> 3) * seq_local + (row & (PADDED - 1)))
    )
    slot = lax.broadcasted_iota(jnp.int32, (count, columns), 0) & (PADDED - 1)
    values = dot(spread_rows, tok_ref[...])
    values = jnp.where(slot == seq_local, 1.0, values)
    own = slot[:, :1] < seq_local
    block_mean = jnp.where(own, jnp.sum(values, axis=1, keepdims=True) * (1.0 / columns), 0.0)
    offsets = values - block_mean
    moment = jnp.where(own, jnp.sum(offsets * offsets, axis=1, keepdims=True), 0.0)
    gain_row = gain_ref[:, ours]
    down, across = grid_index((columns, columns))
    gain_col = jnp.sum(jnp.where(down == across, gain_row, 0.0), axis=1, keepdims=True)
    exact = values.astype(BF16)
    parts = []
    for ref in (wq, wk, wv, wo):
        high, low = rounded_pieces(ref[...].astype(F32) * gain_col, 2)
        parts.append(dot(exact, high.astype(BF16)) + dot(exact, low.astype(BF16)))
    product = jnp.concatenate(parts, axis=1)
    tiles = product.reshape(blocks, PADDED, product.shape[1])
    sums = tiles[:, seq_local : seq_local + 1, :]
    centred = tiles - block_mean.reshape(blocks, PADDED, 1) * sums

    pick, _ = grid_index((wi.shape[0], columns))

    def gate_part(ref):
        chosen = jnp.sum(jnp.where(pick == head, ref[:, ours].astype(F32), 0.0), axis=0, keepdims=True)
        return jnp.sum(offsets * (chosen * gain_row), axis=1, keepdims=True)

    gates = [*rounded_pieces(gate_part(wi), 2), *rounded_pieces(gate_part(wf), 2)]
    lane = lax.broadcasted_iota(jnp.int32, (count, LANES), 1)
    start = jnp.where(slot[:, :1] == seq_local, GATE_SUMS, 0)
    table = jnp.zeros((count, LANES), F32)
    for k, piece in enumerate(gates):
        table = jnp.where(lane == start + k, piece, table)
    table = jnp.where(slot == PADDED - 1, 0.0, table)
    for k, piece in enumerate([*rounded_pieces(block_mean, 3), *rounded_pieces(moment, 2)]):
        table = jnp.where((lane == 4 + k) & own, piece, table)
    exact_table = table.astype(BF16)
    down, across = grid_index((count, count))
    same = (down >> 3) == (across >> 3)
    last = (down & (PADDED - 1)) == PADDED - 1
    inner = across & (PADDED - 1)
    laid = []
    for r in range(seq_local):
        laid.append(dot(one_hot(same & last & ((inner == r) | (inner == seq_local))), exact_table))
    side = jnp.concatenate(laid, axis=1).reshape(tiles.shape)
    out_ref[...] = (centred + side).astype(BF16)


def receive_kernel(
    in_bias, for_bias, got_ref, cell_ref, norm_ref, max_ref, gain_ref,
    mixed_ref, keep_ref, admit_ref, value_ref, norm_out, max_out, *, columns
):
    head = lax.axis_index("tp")
    blocks, padded, width = got_ref.shape
    seq_local, _, key_size, value_size = cell_ref.shape
    count = blocks * padded
    got = got_ref[...].astype(F32)
    flat = got.reshape(count, width).astype(BF16)
    down, across = grid_index((count, count))
    same = (down >> 3) == (across >> 3)
    inner = across & (PADDED - 1)
    outer = down & (PADDED - 1)
    table = jnp.zeros((count, LANES), F32)
    for r in range(seq_local):
        back = one_hot(same & (outer == r) & (inner == PADDED - 1))
        table = table + dot(back, flat[:, r * LANES : (r + 1) * LANES])
    sums = dot(one_hot(same & (inner == seq_local)), flat).reshape(blocks, padded, width)
    lane = lax.broadcasted_iota(jnp.int32, (count, LANES), 1)

    def lanes(first, number):
        kept = jnp.where((lane >= first) & (lane < first + number), table, 0.0)
        return jnp.sum(kept, axis=1, keepdims=True).reshape(blocks, padded, 1)

    means = lanes(4, 3)
    row_mean = jnp.sum(means, axis=0, keepdims=True) * (1.0 / blocks)
    shifts = means - row_mean
    spread = jnp.sum(lanes(7, 2) + columns * shifts * shifts, axis=0) * (1.0 / (blocks * columns))
    inv_scale = lax.rsqrt(spread + NORM_EPS)
    projected = inv_scale * jnp.sum(got + shifts * sums, axis=0)

    def rounded(a, b):
        return projected[:, a:b].astype(BF16).astype(F32)

    query = rounded(0, key_size) * key_size**-0.5
    key = rounded(key_size, 2 * key_size)
    value = rounded(2 * key_size, 2 * key_size + value_size)
    outgate = rounded(2 * key_size + value_size, width)
    input_pre = (
        inv_scale * jnp.sum(lanes(0, 2) + shifts * lanes(GATE_SUMS, 2), axis=0) + in_bias[head]
    )
    forget_pre = (
        inv_scale * jnp.sum(lanes(2, 2) + shifts * lanes(GATE_SUMS + 2, 2), axis=0)
        + for_bias[head]
    )
    down, across = grid_index((padded, seq_local))
    old_max = jnp.sum(jnp.where(down == across, max_ref[...], 0.0), axis=1, keepdims=True)
    log_forget = jnp.minimum(forget_pre, 0.0) - jnp.log1p(jnp.exp(-jnp.abs(forget_pre)))
    carried = log_forget + old_max
    new_max = jnp.maximum(carried, input_pre)
    keep_old = jnp.exp(carried - new_max)
    admit_key = jnp.exp(input_pre - new_max) * key
    max_out[...] = new_max[:seq_local]
    keep_ref[...] = keep_old[:seq_local]
    admit_ref[...] = admit_key[:seq_local]
    value_ref[...] = value[:seq_local]
    query_cols = query.T
    rows = lax.broadcasted_iota(jnp.int32, (padded, value_size), 0)
    against_cell = jnp.zeros((padded, value_size), F32)
    for s in range(seq_local):
        norm_out[s : s + 1] = keep_old[s : s + 1] * norm_ref[s] + admit_key[s : s + 1]
        read = jnp.sum(query_cols[:, s : s + 1] * cell_ref[s, 0], axis=0, keepdims=True)
        against_cell = jnp.where(rows == s, read, against_cell)
    scores = jnp.sum(query * admit_key, axis=1, keepdims=True)
    readout = jnp.where(rows < seq_local, keep_old * against_cell + scores * value, 0.0)
    outgate = jnp.where(rows < seq_local, outgate, 0.0)
    head_mean = jnp.mean(readout, axis=1, keepdims=True)
    around = readout - head_mean
    head_var = jnp.mean(around * around, axis=1, keepdims=True)
    gain = gain_ref[:, pl.ds(pl.multiple_of(head * value_size, LANES), value_size)]
    opened = 1.0 / (1.0 + jnp.exp(-outgate))
    mixed = around * lax.rsqrt(head_var + HEAD_EPS) * gain * opened
    mixed_ref[...] = jnp.broadcast_to(mixed[None], (blocks, padded, value_size)).astype(BF16)


def project_kernel(got_ref, weight_ref, out_ref, *, seq_local):
    blocks, padded, width = got_ref.shape
    seq_total = out_ref.shape[1]
    rows = got_ref[...].astype(F32).reshape(blocks * padded, width).astype(BF16)
    terms = dot(rows, weight_ref[...]).astype(BF16)
    row, col = grid_index((seq_total, blocks * padded))
    inner = col & (PADDED - 1)
    packed = dot(one_hot((inner < seq_local) & (row == (col >> 3) * seq_local + inner)), terms)
    out_ref[...] = jnp.broadcast_to(packed.astype(BF16)[None], out_ref.shape)


def pair_kernel(got_ref, out_ref):
    added = (got_ref[0].astype(F32) + got_ref[1].astype(F32)).astype(BF16)
    out_ref[...] = jnp.broadcast_to(added[None], out_ref.shape)


def stream_kernel(got_ref, tok_ref, picker_ref, stream_ref, out_ref):
    mixer_out = jnp.sum(got_ref[...].astype(F32), axis=0)
    stream = (tok_ref[...].astype(F32) + mixer_out).astype(BF16)
    stream_ref[...] = stream
    chosen = lax.dot_general(
        picker_ref[...], stream, (((0,), (0,)), ((), ())), preferred_element_type=F32
    )
    out_ref[...] = chosen.astype(BF16).reshape(out_ref.shape)


def expert_kernel(
    up_hbm, down_hbm, got_ref, gain_ref, gate_ref, out_ref, up_ref, down_ref, arrived
):
    fetches = [
        pltpu.make_async_copy(up_hbm, up_ref, arrived.at[0]),
        pltpu.make_async_copy(down_hbm, down_ref, arrived.at[1]),
    ]
    for fetch in fetches:
        fetch.start()
    blocks, _, columns = got_ref.shape
    values = jnp.concatenate([got_ref[e].astype(F32) for e in range(blocks)], axis=1)
    row_mean = jnp.mean(values, axis=1, keepdims=True)
    spread = jnp.mean(values * values, axis=1, keepdims=True) - row_mean * row_mean
    normed = ((values - row_mean) * lax.rsqrt(spread + NORM_EPS) * gain_ref[...]).astype(BF16)
    gate = dot(normed, gate_ref[0])
    fetches[0].wait()
    active = (gate / (1.0 + jnp.exp(-gate)) * dot(normed, up_ref[0])).astype(BF16)
    fetches[1].wait()
    result = dot(active, down_ref[0]).astype(BF16)
    for e in range(blocks):
        out_ref[e] = result[:, e * columns : (e + 1) * columns]


def combine_kernel(table_ref, back_ref, out_ref):
    seq_total = out_ref.shape[1]
    experts, slots, columns = back_ref.shape
    both = dot(table_ref[...], back_ref[...].reshape(experts * slots, columns))
    added = (both[:seq_total] + both[seq_total:]).astype(BF16)
    out_ref[...] = jnp.broadcast_to(added[None], out_ref.shape)


def in_vmem(array):
    return pltpu.with_memory_space_constraint(array, pltpu.VMEM)


def kernel_call(kernel, name, shapes, near, scalars=(), far=(), left=(), scratch=()):
    vmem = pl.BlockSpec(memory_space=pltpu.VMEM)
    smem = pl.BlockSpec(memory_space=pltpu.SMEM)
    return pl.pallas_call(
        kernel,
        in_specs=[smem] * len(scalars)
        + [pl.BlockSpec(memory_space=pl.ANY)] * len(left)
        + [vmem] * (len(far) + len(near)),
        out_specs=jax.tree.map(lambda _: vmem, shapes),
        out_shape=shapes,
        scratch_shapes=scratch,
        name=name,
    )(*scalars, *left, *far, *(in_vmem(a) for a in near))


def on_device(
    tokens,
    first_gain,
    w_query,
    w_key,
    w_value,
    w_outgate,
    w_input,
    w_forget,
    input_bias,
    forget_bias,
    head_gain,
    w_project,
    cell_state,
    norm_state,
    max_state,
    second_gain,
    routes,
    route_weight,
    expert_gate,
    expert_up,
    expert_down,
):
    blocks = lax.axis_size("ep")
    seq_total, columns = tokens.shape
    seq_local = seq_total // blocks
    value_size = cell_state.shape[3]
    experts = blocks
    slot_count = blocks * CAPACITY
    expert_ids = lax.broadcasted_iota(jnp.int32, (1, 1, experts), 2)
    matches = routes[:, :, None] == expert_ids
    routed = jnp.sum(matches.astype(jnp.int32), axis=1)
    combine = jnp.sum(jnp.where(matches, route_weight[:, :, None], 0.0), axis=1)
    running = (
        jnp.cumsum(routed.reshape(blocks, seq_local, experts), axis=1).reshape(seq_total, experts)
        - routed
    )
    block_ids = lax.broadcasted_iota(jnp.int32, (seq_total, experts), 0) // seq_local
    slot_of = block_ids * CAPACITY + running
    slot_ids = lax.broadcasted_iota(jnp.int32, (experts, slot_count, seq_total), 1)
    placed = (slot_of.T[:, None, :] == slot_ids) & (routed.T[:, None, :] > 0)
    picker = placed.astype(BF16).reshape(experts * slot_count, seq_total).T
    weighted = jnp.where(placed, combine.T[:, None, :], 0.0)

    width = 2 * (w_query.shape[1] + w_value.shape[1])
    outgoing, old_max = kernel_call(
        functools.partial(send_kernel, seq_local=seq_local),
        "send_parts",
        [pltpu.VMEM((blocks, PADDED, width), BF16), pltpu.VMEM((1, seq_local), F32)],
        (),
        far=(
            tokens,
            first_gain.reshape(1, -1),
            w_query,
            w_key,
            w_value,
            w_outgate,
            w_input.T,
            w_forget.T,
            max_state.T,
        ),
    )
    weight_rows = weighted.reshape(experts * slot_count, seq_total).T
    table = jnp.concatenate([t.astype(BF16) for t in in_pieces(weight_rows, 2)], axis=0)
    incoming, picker, table = lax.optimization_barrier((exchanged(outgoing, "ep"), picker, table))

    key_size = cell_state.shape[2]
    mixed, *updates = kernel_call(
        functools.partial(receive_kernel, columns=columns),
        "cell_step",
        [
            pltpu.VMEM((blocks, PADDED, value_size), BF16),
            pltpu.VMEM((seq_local, 1), F32),
            pltpu.VMEM((seq_local, key_size), F32),
            pltpu.VMEM((seq_local, value_size), F32),
            pltpu.VMEM((seq_local, key_size), F32),
            pltpu.VMEM((seq_local, 1), F32),
        ],
        (incoming, cell_state, norm_state, old_max, head_gain.reshape(1, -1)),
        scalars=(input_bias, forget_bias),
    )

    part_shape = pltpu.VMEM((2, seq_total, columns), BF16)
    chip_shape = pltpu.VMEM((lax.axis_size("tp") // 2, seq_total, columns), BF16)
    head_terms = kernel_call(
        functools.partial(project_kernel, seq_local=seq_local),
        "project_heads",
        part_shape,
        (exchanged(mixed, "ep"), w_project),
    )
    chip_terms = kernel_call(
        pair_kernel, "chip_heads", chip_shape, (swapped(head_terms, cores_of_chips("tp")),)
    )
    stream, outbound = kernel_call(
        stream_kernel,
        "stream_rows",
        [
            pltpu.VMEM(tokens.shape, BF16),
            pltpu.VMEM((experts, slot_count, columns), BF16),
        ],
        (swapped(chip_terms, chips_of_cores("tp")), tokens, picker),
    )

    slot_out = kernel_call(
        expert_kernel,
        "expert",
        pltpu.VMEM((blocks, slot_count, columns), BF16),
        (
            exchanged(outbound, "ep"),
            second_gain.reshape(1, -1),
            expert_gate,
        ),
        left=(expert_up, expert_down),
        scratch=(
            pltpu.VMEM(expert_up.shape, BF16),
            pltpu.VMEM(expert_down.shape, BF16),
            pltpu.SemaphoreType.DMA((2,)),
        ),
    )
    moe_terms = kernel_call(
        combine_kernel, "combine", part_shape, (table, exchanged(slot_out, "ep"))
    )
    moe_terms = kernel_call(
        pair_kernel, "chip_moe", chip_shape, (swapped(moe_terms, cores_of_chips("tp")),)
    )
    moe_terms, *updates = lax.optimization_barrier((moe_terms, *updates))
    keep_old, admit_key, value, new_norm, new_max = updates
    new_cell = (
        keep_old[:, :, None] * cell_state[:, 0] + admit_key[:, :, None] * value[:, None, :]
    )
    moe_out = jnp.sum(swapped(moe_terms, chips_of_cores("tp")).astype(F32), axis=0)
    layer_out = (stream.astype(F32) + moe_out).astype(BF16)
    return (layer_out, new_cell[:, None], new_norm[:, None], new_max)


def solution(mesh):
    placed = (
        P("grp", "ep"),
        P(),
        P("ep", "tp"),
        P("ep", "tp"),
        P("ep", "tp"),
        P("ep", "tp"),
        P(),
        P(),
        P(),
        P(),
        P(),
        P("tp", "ep"),
        P(("grp", "ep"), "tp", None, None),
        P(("grp", "ep"), "tp", None),
        P(("grp", "ep"), "tp"),
        P(),
        P("grp", None),
        P("grp", None),
        P("ep", None, "tp"),
        P("ep", None, "tp"),
        P("ep", "tp", None),
    )
    return jax.shard_map(
        on_device,
        mesh=mesh,
        in_specs=placed,
        out_specs=(
            P("grp", "ep"),
            P(("grp", "ep"), "tp", None, None),
            P(("grp", "ep"), "tp", None),
            P(("grp", "ep"), "tp"),
        ),
        check_vma=False,
    )
```

```python
import functools

import jax
import jax.numpy as jnp
from jax import lax
from jax.experimental import pallas as pl
from jax.experimental.pallas import tpu as pltpu
from jax.sharding import PartitionSpec as P

NORM_EPS = 1e-05
HEAD_EPS = 1e-06
CAPACITY = 2
LANES = 128
PADDED = 8
GATE_SUMS = 16
F32 = jnp.float32
BF16 = jnp.bfloat16


def exchanged(blocks, axis):
    return lax.all_to_all(blocks, axis, split_axis=0, concat_axis=0, tiled=True)


def from_other_core(array):
    size = lax.axis_size("tp")
    return lax.ppermute(array, "tp", [(i, i ^ 1) for i in range(size)])


def chips_of_cores(axis):
    size = lax.axis_size(axis)
    return [list(range(core, size, 2)) for core in range(2)]


def swapped(blocks, groups):
    return lax.all_to_all(
        blocks, "tp", split_axis=0, concat_axis=0, tiled=True, axis_index_groups=groups
    )


def in_pieces(values, count):
    pieces = []
    for _ in range(count - 1):
        head = lax.reduce_precision(values, 8, 7)
        pieces.append(head)
        values = values - head
    pieces.append(values)
    return pieces


def rounded_pieces(values, count):
    pieces = []
    for _ in range(count):
        head = values.astype(BF16).astype(F32)
        pieces.append(head)
        values = values - head
    return pieces


def dot(a, b):
    return jnp.dot(a, b, preferred_element_type=F32)


def grid_index(shape):
    return lax.broadcasted_iota(jnp.int32, shape, 0), lax.broadcasted_iota(jnp.int32, shape, 1)


def one_hot(condition):
    return jnp.where(condition, 1.0, 0.0).astype(BF16)


def send_kernel(
    tok_ref, gain_ref, wq, wk, wv, wo, wi, wf, max_ref, out_ref, max_out, *, seq_local
):
    max_out[...] = max_ref[...]
    head = lax.axis_index("tp")
    seq_total, columns = tok_ref.shape
    ours = pl.ds(pl.multiple_of(lax.axis_index("ep") * columns, LANES), columns)
    blocks = seq_total // seq_local
    count = blocks * PADDED
    row, col = grid_index((count, seq_total))
    spread_rows = one_hot(
        ((row & (PADDED - 1)) < seq_local)
        & (col == (row >> 3) * seq_local + (row & (PADDED - 1)))
    )
    slot = lax.broadcasted_iota(jnp.int32, (count, columns), 0) & (PADDED - 1)
    values = dot(spread_rows, tok_ref[...])
    values = jnp.where(slot == seq_local, 1.0, values)
    own = slot[:, :1] < seq_local
    block_mean = jnp.where(own, jnp.sum(values, axis=1, keepdims=True) * (1.0 / columns), 0.0)
    offsets = values - block_mean
    moment = jnp.where(own, jnp.sum(offsets * offsets, axis=1, keepdims=True), 0.0)
    gain_row = gain_ref[:, ours]
    down, across = grid_index((columns, columns))
    gain_col = jnp.sum(jnp.where(down == across, gain_row, 0.0), axis=1, keepdims=True)
    exact = jnp.concatenate([values.astype(BF16)] * 2, axis=1)
    parts = []
    for ref in (wq, wk, wv, wo):
        pieces = rounded_pieces(ref[...].astype(F32) * gain_col, 2)
        parts.append(dot(exact, jnp.concatenate([p.astype(BF16) for p in pieces], axis=0)))
    product = jnp.concatenate(parts, axis=1)
    tiles = product.reshape(blocks, PADDED, product.shape[1])
    sums = tiles[:, seq_local : seq_local + 1, :]
    centred = tiles - block_mean.reshape(blocks, PADDED, 1) * sums

    pick, _ = grid_index((wi.shape[0], columns))

    def gate_part(ref):
        chosen = jnp.sum(jnp.where(pick == head, ref[:, ours].astype(F32), 0.0), axis=0, keepdims=True)
        return jnp.sum(offsets * (chosen * gain_row), axis=1, keepdims=True)

    gates = [*rounded_pieces(gate_part(wi), 2), *rounded_pieces(gate_part(wf), 2)]
    lane = lax.broadcasted_iota(jnp.int32, (count, LANES), 1)
    start = jnp.where(slot[:, :1] == seq_local, GATE_SUMS, 0)
    table = jnp.zeros((count, LANES), F32)
    for k, piece in enumerate(gates):
        table = jnp.where(lane == start + k, piece, table)
    table = jnp.where(slot == PADDED - 1, 0.0, table)
    for k, piece in enumerate([*rounded_pieces(block_mean, 3), *rounded_pieces(moment, 2)]):
        table = jnp.where((lane == 4 + k) & own, piece, table)
    exact_table = table.astype(BF16)
    down, across = grid_index((count, count))
    same = (down >> 3) == (across >> 3)
    last = (down & (PADDED - 1)) == PADDED - 1
    inner = across & (PADDED - 1)
    moves = [
        one_hot(same & last & ((inner == r) | (inner == seq_local))) for r in range(seq_local)
    ]
    laid = dot(jnp.concatenate(moves, axis=0), exact_table)
    side = jnp.concatenate(
        [laid[r * count : (r + 1) * count] for r in range(seq_local)], axis=1
    ).reshape(tiles.shape)
    out_ref[...] = (centred + side).astype(BF16)


def receive_kernel(
    in_bias, for_bias, got_ref, cell_ref, norm_ref, max_ref, gain_ref,
    mixed_ref, keep_ref, admit_ref, value_ref, norm_out, max_out, *, columns
):
    head = lax.axis_index("tp")
    blocks, padded, width = got_ref.shape
    seq_local, _, key_size, value_size = cell_ref.shape
    count = blocks * padded
    got = got_ref[...].astype(F32)
    flat = got.reshape(count, width).astype(BF16)
    down, across = grid_index((count, count))
    same = (down >> 3) == (across >> 3)
    inner = across & (PADDED - 1)
    outer = down & (PADDED - 1)
    moves = [
        one_hot(same & (outer == r) & (inner == PADDED - 1)) for r in range(seq_local)
    ]
    table = dot(
        jnp.concatenate(moves, axis=1),
        jnp.concatenate([flat[:, r * LANES : (r + 1) * LANES] for r in range(seq_local)], axis=0),
    )
    sums = got[:, seq_local : seq_local + 1, :]
    lane = lax.broadcasted_iota(jnp.int32, (count, LANES), 1)

    def lanes(first, number):
        kept = jnp.where((lane >= first) & (lane < first + number), table, 0.0)
        return jnp.sum(kept, axis=1, keepdims=True).reshape(blocks, padded, 1)

    means = lanes(4, 3)
    row_mean = jnp.sum(means, axis=0, keepdims=True) * (1.0 / blocks)
    shifts = means - row_mean
    spread = jnp.sum(lanes(7, 2) + columns * shifts * shifts, axis=0) * (1.0 / (blocks * columns))
    inv_scale = lax.rsqrt(spread + NORM_EPS)
    projected = inv_scale * jnp.sum(got + shifts * sums, axis=0)

    def rounded(a, b):
        return projected[:, a:b].astype(BF16).astype(F32)

    query = rounded(0, key_size) * key_size**-0.5
    key = rounded(key_size, 2 * key_size)
    value = rounded(2 * key_size, 2 * key_size + value_size)
    outgate = rounded(2 * key_size + value_size, width)
    input_pre = (
        inv_scale * jnp.sum(lanes(0, 2) + shifts * lanes(GATE_SUMS, 2), axis=0) + in_bias[head]
    )
    forget_pre = (
        inv_scale * jnp.sum(lanes(2, 2) + shifts * lanes(GATE_SUMS + 2, 2), axis=0)
        + for_bias[head]
    )
    down, across = grid_index((padded, seq_local))
    old_max = jnp.sum(jnp.where(down == across, max_ref[...], 0.0), axis=1, keepdims=True)
    log_forget = jnp.minimum(forget_pre, 0.0) - jnp.log1p(jnp.exp(-jnp.abs(forget_pre)))
    carried = log_forget + old_max
    new_max = jnp.maximum(carried, input_pre)
    keep_old = jnp.exp(carried - new_max)
    admit_key = jnp.exp(input_pre - new_max) * key
    max_out[...] = new_max[:seq_local]
    keep_ref[...] = keep_old[:seq_local]
    admit_ref[...] = admit_key[:seq_local]
    value_ref[...] = value[:seq_local]
    query_cols = query.T
    rows = lax.broadcasted_iota(jnp.int32, (padded, value_size), 0)
    against_cell = jnp.zeros((padded, value_size), F32)
    for s in range(seq_local):
        norm_out[s : s + 1] = keep_old[s : s + 1] * norm_ref[s] + admit_key[s : s + 1]
        read = jnp.sum(query_cols[:, s : s + 1] * cell_ref[s, 0], axis=0, keepdims=True)
        against_cell = jnp.where(rows == s, read, against_cell)
    scores = jnp.sum(query * admit_key, axis=1, keepdims=True)
    readout = jnp.where(rows < seq_local, keep_old * against_cell + scores * value, 0.0)
    outgate = jnp.where(rows < seq_local, outgate, 0.0)
    head_mean = jnp.mean(readout, axis=1, keepdims=True)
    around = readout - head_mean
    head_var = jnp.mean(around * around, axis=1, keepdims=True)
    gain = gain_ref[:, pl.ds(pl.multiple_of(head * value_size, LANES), value_size)]
    opened = 1.0 / (1.0 + jnp.exp(-outgate))
    mixed = around * lax.rsqrt(head_var + HEAD_EPS) * gain * opened
    mixed_ref[...] = jnp.broadcast_to(mixed[None], (blocks, padded, value_size)).astype(BF16)


def project_kernel(got_ref, weight_ref, out_ref, *, seq_local):
    blocks, padded, width = got_ref.shape
    seq_total = out_ref.shape[0]
    rows = got_ref[...].astype(F32).reshape(blocks * padded, width).astype(BF16)
    terms = dot(rows, weight_ref[...]).astype(BF16)
    row, col = grid_index((seq_total, blocks * padded))
    inner = col & (PADDED - 1)
    packed = dot(one_hot((inner < seq_local) & (row == (col >> 3) * seq_local + inner)), terms)
    out_ref[...] = packed.astype(BF16)


def pair_kernel(own_ref, other_ref, out_ref):
    added = (own_ref[...].astype(F32) + other_ref[...].astype(F32)).astype(BF16)
    out_ref[...] = jnp.broadcast_to(added[None], out_ref.shape)


def stream_kernel(got_ref, tok_ref, picker_ref, stream_ref, out_ref):
    mixer_out = jnp.sum(got_ref[...].astype(F32), axis=0)
    stream = (tok_ref[...].astype(F32) + mixer_out).astype(BF16)
    stream_ref[...] = stream
    chosen = lax.dot_general(
        picker_ref[...], stream, (((0,), (0,)), ((), ())), preferred_element_type=F32
    )
    out_ref[...] = chosen.astype(BF16).reshape(out_ref.shape)


def expert_kernel(
    up_hbm, down_hbm, got_ref, gain_ref, gate_ref, out_ref, up_ref, down_ref, arrived
):
    fetches = [
        pltpu.make_async_copy(up_hbm, up_ref, arrived.at[0]),
        pltpu.make_async_copy(down_hbm, down_ref, arrived.at[1]),
    ]
    for fetch in fetches:
        fetch.start()
    blocks, _, columns = got_ref.shape
    values = jnp.concatenate([got_ref[e].astype(F32) for e in range(blocks)], axis=1)
    row_mean = jnp.mean(values, axis=1, keepdims=True)
    spread = jnp.mean(values * values, axis=1, keepdims=True) - row_mean * row_mean
    normed = ((values - row_mean) * lax.rsqrt(spread + NORM_EPS) * gain_ref[...]).astype(BF16)
    gate = dot(normed, gate_ref[0])
    fetches[0].wait()
    active = (gate / (1.0 + jnp.exp(-gate)) * dot(normed, up_ref[0])).astype(BF16)
    fetches[1].wait()
    result = dot(active, down_ref[0]).astype(BF16)
    for e in range(blocks):
        out_ref[e] = result[:, e * columns : (e + 1) * columns]


def combine_kernel(table_ref, back_ref, out_ref):
    seq_total = out_ref.shape[0]
    experts, slots, columns = back_ref.shape
    both = dot(table_ref[...], back_ref[...].reshape(experts * slots, columns))
    out_ref[...] = (both[:seq_total] + both[seq_total:]).astype(BF16)


def in_vmem(array):
    return pltpu.with_memory_space_constraint(array, pltpu.VMEM)


def kernel_call(kernel, name, shapes, near, scalars=(), far=(), left=(), scratch=()):
    vmem = pl.BlockSpec(memory_space=pltpu.VMEM)
    smem = pl.BlockSpec(memory_space=pltpu.SMEM)
    return pl.pallas_call(
        kernel,
        in_specs=[smem] * len(scalars)
        + [pl.BlockSpec(memory_space=pl.ANY)] * len(left)
        + [vmem] * (len(far) + len(near)),
        out_specs=jax.tree.map(lambda _: vmem, shapes),
        out_shape=shapes,
        scratch_shapes=scratch,
        name=name,
    )(*scalars, *left, *far, *(in_vmem(a) for a in near))


def on_device(
    tokens,
    first_gain,
    w_query,
    w_key,
    w_value,
    w_outgate,
    w_input,
    w_forget,
    input_bias,
    forget_bias,
    head_gain,
    w_project,
    cell_state,
    norm_state,
    max_state,
    second_gain,
    routes,
    route_weight,
    expert_gate,
    expert_up,
    expert_down,
):
    blocks = lax.axis_size("ep")
    seq_total, columns = tokens.shape
    seq_local = seq_total // blocks
    value_size = cell_state.shape[3]
    experts = blocks
    slot_count = blocks * CAPACITY
    expert_ids = lax.broadcasted_iota(jnp.int32, (1, 1, experts), 2)
    matches = routes[:, :, None] == expert_ids
    routed = jnp.sum(matches.astype(jnp.int32), axis=1)
    combine = jnp.sum(jnp.where(matches, route_weight[:, :, None], 0.0), axis=1)
    running = (
        jnp.cumsum(routed.reshape(blocks, seq_local, experts), axis=1).reshape(seq_total, experts)
        - routed
    )
    block_ids = lax.broadcasted_iota(jnp.int32, (seq_total, experts), 0) // seq_local
    slot_of = block_ids * CAPACITY + running
    slot_ids = lax.broadcasted_iota(jnp.int32, (experts, slot_count, seq_total), 1)
    placed = (slot_of.T[:, None, :] == slot_ids) & (routed.T[:, None, :] > 0)
    picker = placed.astype(BF16).reshape(experts * slot_count, seq_total).T
    weighted = jnp.where(placed, combine.T[:, None, :], 0.0)

    width = 2 * (w_query.shape[1] + w_value.shape[1])
    outgoing, old_max = kernel_call(
        functools.partial(send_kernel, seq_local=seq_local),
        "send_parts",
        [pltpu.VMEM((blocks, PADDED, width), BF16), pltpu.VMEM((1, seq_local), F32)],
        (),
        far=(
            tokens,
            first_gain.reshape(1, -1),
            w_query,
            w_key,
            w_value,
            w_outgate,
            w_input.T,
            w_forget.T,
            max_state.T,
        ),
    )
    weight_rows = weighted.reshape(experts * slot_count, seq_total).T
    table = jnp.concatenate([t.astype(BF16) for t in in_pieces(weight_rows, 2)], axis=0)
    incoming, picker, table = lax.optimization_barrier((exchanged(outgoing, "ep"), picker, table))

    key_size = cell_state.shape[2]
    mixed, *updates = kernel_call(
        functools.partial(receive_kernel, columns=columns),
        "cell_step",
        [
            pltpu.VMEM((blocks, PADDED, value_size), BF16),
            pltpu.VMEM((seq_local, 1), F32),
            pltpu.VMEM((seq_local, key_size), F32),
            pltpu.VMEM((seq_local, value_size), F32),
            pltpu.VMEM((seq_local, key_size), F32),
            pltpu.VMEM((seq_local, 1), F32),
        ],
        (incoming, cell_state, norm_state, old_max, head_gain.reshape(1, -1)),
        scalars=(input_bias, forget_bias),
    )

    part_shape = pltpu.VMEM((seq_total, columns), BF16)
    chip_shape = pltpu.VMEM((lax.axis_size("tp") // 2, seq_total, columns), BF16)
    head_terms = kernel_call(
        functools.partial(project_kernel, seq_local=seq_local),
        "project_heads",
        part_shape,
        (exchanged(mixed, "ep"), w_project),
    )
    chip_terms = kernel_call(
        pair_kernel, "chip_heads", chip_shape, (head_terms, from_other_core(head_terms))
    )
    stream, outbound = kernel_call(
        stream_kernel,
        "stream_rows",
        [
            pltpu.VMEM(tokens.shape, BF16),
            pltpu.VMEM((experts, slot_count, columns), BF16),
        ],
        (swapped(chip_terms, chips_of_cores("tp")), tokens, picker),
    )

    slot_out = kernel_call(
        expert_kernel,
        "expert",
        pltpu.VMEM((blocks, slot_count, columns), BF16),
        (
            exchanged(outbound, "ep"),
            second_gain.reshape(1, -1),
            expert_gate,
        ),
        left=(expert_up, expert_down),
        scratch=(
            pltpu.VMEM(expert_up.shape, BF16),
            pltpu.VMEM(expert_down.shape, BF16),
            pltpu.SemaphoreType.DMA((2,)),
        ),
    )
    moe_terms = kernel_call(
        combine_kernel, "combine", part_shape, (table, exchanged(slot_out, "ep"))
    )
    moe_terms = kernel_call(
        pair_kernel, "chip_moe", chip_shape, (moe_terms, from_other_core(moe_terms))
    )
    moe_terms, *updates = lax.optimization_barrier((moe_terms, *updates))
    keep_old, admit_key, value, new_norm, new_max = updates
    new_cell = (
        keep_old[:, :, None] * cell_state[:, 0] + admit_key[:, :, None] * value[:, None, :]
    )
    moe_out = jnp.sum(swapped(moe_terms, chips_of_cores("tp")).astype(F32), axis=0)
    layer_out = (stream.astype(F32) + moe_out).astype(BF16)
    return (layer_out, new_cell[:, None], new_norm[:, None], new_max)


def solution(mesh):
    placed = (
        P("grp", "ep"),
        P(),
        P("ep", "tp"),
        P("ep", "tp"),
        P("ep", "tp"),
        P("ep", "tp"),
        P(),
        P(),
        P(),
        P(),
        P(),
        P("tp", "ep"),
        P(("grp", "ep"), "tp", None, None),
        P(("grp", "ep"), "tp", None),
        P(("grp", "ep"), "tp"),
        P(),
        P("grp", None),
        P("grp", None),
        P("ep", None, "tp"),
        P("ep", None, "tp"),
        P("ep", "tp", None),
    )
    return jax.shard_map(
        on_device,
        mesh=mesh,
        in_specs=placed,
        out_specs=(
            P("grp", "ep"),
            P(("grp", "ep"), "tp", None, None),
            P(("grp", "ep"), "tp", None),
            P(("grp", "ep"), "tp"),
        ),
        check_vma=False,
    )
```

```python
import functools

import jax
import jax.numpy as jnp
from jax import lax
from jax.experimental import pallas as pl
from jax.experimental.pallas import tpu as pltpu
from jax.sharding import PartitionSpec as P

NORM_EPS = 1e-05
HEAD_EPS = 1e-06
CAPACITY = 2
LANES = 128
PADDED = 8
GATE_SUMS = 16
F32 = jnp.float32
BF16 = jnp.bfloat16


def exchanged(blocks, axis):
    return lax.all_to_all(blocks, axis, split_axis=0, concat_axis=0, tiled=True)


def from_other_core(array):
    size = lax.axis_size("tp")
    return lax.ppermute(array, "tp", [(i, i ^ 1) for i in range(size)])


def chips_of_cores(axis):
    size = lax.axis_size(axis)
    return [list(range(core, size, 2)) for core in range(2)]


def swapped(blocks, groups):
    return lax.all_to_all(
        blocks, "tp", split_axis=0, concat_axis=0, tiled=True, axis_index_groups=groups
    )


def rounded_pieces(values, count):
    pieces = []
    for _ in range(count):
        head = values.astype(BF16).astype(F32)
        pieces.append(head)
        values = values - head
    return pieces


def dot(a, b):
    return jnp.dot(a, b, preferred_element_type=F32)


def lane_sums(values, count):
    ones = jnp.ones((values.shape[1], LANES), BF16)
    return sum(dot(piece.astype(BF16), ones) for piece in rounded_pieces(values, count))


def grid_index(shape):
    return lax.broadcasted_iota(jnp.int32, shape, 0), lax.broadcasted_iota(jnp.int32, shape, 1)


def one_hot(condition):
    return jnp.where(condition, 1.0, 0.0).astype(BF16)


def send_kernel(tok_ref, gain_ref, wq, wk, wv, wo, wi, wf, *rest, seq_local):
    handed = len(rest) // 2
    out_ref = rest[handed]
    for kept, copy in zip(rest[:handed], rest[handed + 1 :]):
        copy[...] = kept[...]
    head = lax.axis_index("tp")
    seq_total, columns = tok_ref.shape
    ours = pl.ds(pl.multiple_of(lax.axis_index("ep") * columns, LANES), columns)
    blocks = seq_total // seq_local
    count = blocks * PADDED
    row, col = grid_index((count, seq_total))
    spread_rows = one_hot(
        ((row & (PADDED - 1)) < seq_local)
        & (col == (row >> 3) * seq_local + (row & (PADDED - 1)))
    )
    slot = lax.broadcasted_iota(jnp.int32, (count, columns), 0) & (PADDED - 1)
    values = dot(spread_rows, tok_ref[...])
    values = jnp.where(slot == seq_local, 1.0, values)
    own = slot < seq_local
    block_mean = jnp.where(own, lane_sums(values, 1) * (1.0 / columns), 0.0)
    offsets = values - block_mean
    moment = jnp.where(own, lane_sums(offsets * offsets, 2), 0.0)
    gain_row = gain_ref[:, ours]
    down, across = grid_index((columns, columns))
    gain_col = lane_sums(jnp.where(down == across, gain_row, 0.0), 3)
    exact = jnp.concatenate([values.astype(BF16)] * 2, axis=1)
    parts = []
    for ref in (wq, wk, wv, wo):
        spread_gain = jnp.concatenate([gain_col] * (ref.shape[1] // LANES), axis=1)
        pieces = rounded_pieces(ref[...].astype(F32) * spread_gain, 2)
        parts.append(dot(exact, jnp.concatenate([p.astype(BF16) for p in pieces], axis=0)))
    product = jnp.concatenate(parts, axis=1)
    tiles = product.reshape(blocks, PADDED, product.shape[1])
    sums = tiles[:, seq_local : seq_local + 1, :]
    wide_mean = jnp.concatenate([block_mean] * (product.shape[1] // LANES), axis=1)
    centred = tiles - wide_mean.reshape(tiles.shape) * sums

    pick, _ = grid_index((wi.shape[0], columns))

    def gate_part(ref):
        chosen = jnp.sum(jnp.where(pick == head, ref[:, ours].astype(F32), 0.0), axis=0, keepdims=True)
        return lane_sums(offsets * (chosen * gain_row), 3)

    gates = [*rounded_pieces(gate_part(wi), 2), *rounded_pieces(gate_part(wf), 2)]
    lane = lax.broadcasted_iota(jnp.int32, (count, LANES), 1)
    start = jnp.where(slot == seq_local, GATE_SUMS, 0)
    table = jnp.zeros((count, LANES), F32)
    for k, piece in enumerate(gates):
        table = jnp.where(lane == start + k, piece, table)
    table = jnp.where(slot == PADDED - 1, 0.0, table)
    for k, piece in enumerate([*rounded_pieces(block_mean, 3), *rounded_pieces(moment, 2)]):
        table = jnp.where((lane == 4 + k) & own, piece, table)
    exact_table = table.astype(BF16)
    down, across = grid_index((count, count))
    same = (down >> 3) == (across >> 3)
    last = (down & (PADDED - 1)) == PADDED - 1
    inner = across & (PADDED - 1)
    moves = [
        one_hot(same & last & ((inner == r) | (inner == seq_local))) for r in range(seq_local)
    ]
    laid = dot(jnp.concatenate(moves, axis=0), exact_table)
    side = jnp.concatenate(
        [laid[r * count : (r + 1) * count] for r in range(seq_local)], axis=1
    ).reshape(tiles.shape)
    out_ref[...] = (centred + side).astype(BF16)


def receive_kernel(
    in_bias, for_bias, cell_hbm, got_ref, norm_ref, max_ref, gain_ref,
    mixed_ref, keep_ref, admit_ref, value_ref, norm_out, max_out, cell_ref, arrived, *, columns
):
    fetch = pltpu.make_async_copy(cell_hbm, cell_ref, arrived)
    fetch.start()
    head = lax.axis_index("tp")
    blocks, padded, width = got_ref.shape
    seq_local, _, key_size, value_size = cell_ref.shape
    count = blocks * padded
    got = got_ref[...].astype(F32)
    flat = got.reshape(count, width).astype(BF16)
    down, across = grid_index((count, count))
    same = (down >> 3) == (across >> 3)
    inner = across & (PADDED - 1)
    outer = down & (PADDED - 1)
    moves = [
        one_hot(same & (outer == r) & (inner == PADDED - 1)) for r in range(seq_local)
    ]
    table = dot(
        jnp.concatenate(moves, axis=1),
        jnp.concatenate([flat[:, r * LANES : (r + 1) * LANES] for r in range(seq_local)], axis=0),
    )
    sums = got[:, seq_local : seq_local + 1, :]
    lane, _ = grid_index((LANES, LANES))
    spans = ((4, 3), (7, 2), (0, 2), (GATE_SUMS, 2), (2, 2), (GATE_SUMS + 2, 2))
    chosen = [one_hot((lane >= first) & (lane < first + number)) for first, number in spans]
    gathered = dot(table.astype(BF16), jnp.concatenate(chosen, axis=1))

    def term(k):
        return gathered[:, k * LANES : (k + 1) * LANES].reshape(blocks, padded, LANES)

    means = term(0)
    row_mean = jnp.sum(means, axis=0, keepdims=True) * (1.0 / blocks)
    shifts = means - row_mean
    spread = jnp.sum(term(1) + columns * shifts * shifts, axis=0) * (1.0 / (blocks * columns))
    inv_scale = lax.rsqrt(spread + NORM_EPS)
    parts = width // LANES
    wide_shifts = jnp.concatenate([shifts] * parts, axis=2)
    projected = jnp.concatenate([inv_scale] * parts, axis=1) * jnp.sum(
        got + wide_shifts * sums, axis=0
    )

    def rounded(a, b):
        return projected[:, a:b].astype(BF16).astype(F32)

    query = rounded(0, key_size) * key_size**-0.5
    key = rounded(key_size, 2 * key_size)
    value = rounded(2 * key_size, 2 * key_size + value_size)
    outgate = rounded(2 * key_size + value_size, width)
    input_pre = (
        inv_scale * jnp.sum(term(2) + shifts * term(3), axis=0) + in_bias[head]
    )
    forget_pre = (
        inv_scale * jnp.sum(term(4) + shifts * term(5), axis=0)
        + for_bias[head]
    )
    down, across = grid_index((padded, seq_local))
    old_max = jnp.sum(jnp.where(down == across, max_ref[...], 0.0), axis=1, keepdims=True)
    log_forget = jnp.minimum(forget_pre, 0.0) - jnp.log1p(jnp.exp(-jnp.abs(forget_pre)))
    carried = log_forget + old_max
    new_max = jnp.maximum(carried, input_pre)
    keep_old = jnp.exp(carried - new_max)
    admit_key = jnp.exp(input_pre - new_max) * key
    max_out[...] = new_max[:seq_local, :1]
    keep_ref[...] = keep_old[:seq_local, :1]
    admit_ref[...] = admit_key[:seq_local]
    value_ref[...] = value[:seq_local]
    query_cols = query.T
    rows = lax.broadcasted_iota(jnp.int32, (padded, value_size), 0)
    against_cell = jnp.zeros((padded, value_size), F32)
    fetch.wait()
    for s in range(seq_local):
        norm_out[s : s + 1] = keep_old[s : s + 1] * norm_ref[s] + admit_key[s : s + 1]
        read = jnp.sum(query_cols[:, s : s + 1] * cell_ref[s, 0], axis=0, keepdims=True)
        against_cell = jnp.where(rows == s, read, against_cell)
    scores = jnp.sum(query * admit_key, axis=1, keepdims=True)
    wide_keep = jnp.concatenate([keep_old] * (value_size // LANES), axis=1)
    readout = jnp.where(rows < seq_local, wide_keep * against_cell + scores * value, 0.0)
    outgate = jnp.where(rows < seq_local, outgate, 0.0)
    head_mean = jnp.mean(readout, axis=1, keepdims=True)
    around = readout - head_mean
    head_var = jnp.mean(around * around, axis=1, keepdims=True)
    gain = gain_ref[:, pl.ds(pl.multiple_of(head * value_size, LANES), value_size)]
    opened = 1.0 / (1.0 + jnp.exp(-outgate))
    mixed = around * lax.rsqrt(head_var + HEAD_EPS) * gain * opened
    mixed_ref[...] = jnp.broadcast_to(mixed[None], (blocks, padded, value_size)).astype(BF16)


def project_kernel(got_ref, weight_ref, out_ref, *, seq_local):
    blocks, padded, width = got_ref.shape
    seq_total = out_ref.shape[0]
    rows = got_ref[...].astype(F32).reshape(blocks * padded, width).astype(BF16)
    terms = dot(rows, weight_ref[...]).astype(BF16)
    row, col = grid_index((seq_total, blocks * padded))
    inner = col & (PADDED - 1)
    packed = dot(one_hot((inner < seq_local) & (row == (col >> 3) * seq_local + inner)), terms)
    out_ref[...] = packed.astype(BF16)


def pair_kernel(own_ref, other_ref, out_ref):
    added = (own_ref[...].astype(F32) + other_ref[...].astype(F32)).astype(BF16)
    out_ref[...] = jnp.broadcast_to(added[None], out_ref.shape)


def column_of(row):
    down, across = grid_index((row.shape[1], row.shape[1]))
    return jnp.sum(jnp.where(down == across, row, 0.0), axis=1, keepdims=True)


def stream_kernel(
    got_ref, tok_ref, route_ref, weight_ref, stream_ref, out_ref, table_ref, *, seq_local
):
    mixer_out = jnp.sum(got_ref[...].astype(F32), axis=0)
    stream = (tok_ref[...].astype(F32) + mixer_out).astype(BF16)
    stream_ref[...] = stream
    top, seq_total = route_ref.shape
    experts, slots, _ = out_ref.shape
    names = [route_ref[k : k + 1].astype(F32) for k in range(top)]
    down, across = grid_index((seq_total, seq_total))
    block_down = jnp.floor((down.astype(F32) + 0.5) * (1.0 / seq_local))
    block_across = jnp.floor((across.astype(F32) + 0.5) * (1.0 / seq_local))
    earlier = (block_down == block_across) & (across < down)
    place = lax.broadcasted_iota(jnp.int32, (seq_total, experts * slots), 1).astype(F32)
    picked = jnp.zeros(place.shape, F32)
    weights = jnp.zeros(place.shape, F32)
    for k in range(top):
        name = column_of(names[k])
        same = sum(jnp.where(earlier & (other == name), 1.0, 0.0) for other in names)
        slot = name * slots + block_down[:, :1] * CAPACITY + jnp.sum(same, axis=1, keepdims=True)
        here = place == slot
        picked = jnp.where(here, 1.0, picked)
        weights = jnp.where(here, column_of(weight_ref[k : k + 1]), weights)
    table = [piece.astype(BF16) for piece in rounded_pieces(weights, 2)]
    table_ref[...] = jnp.concatenate(table, axis=0)
    chosen = lax.dot_general(
        picked.astype(BF16), stream, (((0,), (0,)), ((), ())), preferred_element_type=F32
    )
    out_ref[...] = chosen.astype(BF16).reshape(out_ref.shape)


def expert_kernel(
    up_hbm, down_hbm, got_ref, gain_ref, gate_ref, out_ref, up_ref, down_ref, arrived
):
    fetches = [
        pltpu.make_async_copy(up_hbm, up_ref, arrived.at[0]),
        pltpu.make_async_copy(down_hbm, down_ref, arrived.at[1]),
    ]
    for fetch in fetches:
        fetch.start()
    blocks, _, columns = got_ref.shape
    values = jnp.concatenate([got_ref[e].astype(F32) for e in range(blocks)], axis=1)
    row_mean = jnp.mean(values, axis=1, keepdims=True)
    spread = jnp.mean(values * values, axis=1, keepdims=True) - row_mean * row_mean
    normed = ((values - row_mean) * lax.rsqrt(spread + NORM_EPS) * gain_ref[...]).astype(BF16)
    gate = dot(normed, gate_ref[0])
    fetches[0].wait()
    active = (gate / (1.0 + jnp.exp(-gate)) * dot(normed, up_ref[0])).astype(BF16)
    fetches[1].wait()
    result = dot(active, down_ref[0]).astype(BF16)
    for e in range(blocks):
        out_ref[e] = result[:, e * columns : (e + 1) * columns]


def combine_kernel(table_ref, back_ref, out_ref):
    seq_total = out_ref.shape[0]
    experts, slots, columns = back_ref.shape
    both = dot(table_ref[...], back_ref[...].reshape(experts * slots, columns))
    out_ref[...] = (both[:seq_total] + both[seq_total:]).astype(BF16)


def in_vmem(array):
    return pltpu.with_memory_space_constraint(array, pltpu.VMEM)


def kernel_call(kernel, name, shapes, near, scalars=(), far=(), left=(), scratch=()):
    vmem = pl.BlockSpec(memory_space=pltpu.VMEM)
    smem = pl.BlockSpec(memory_space=pltpu.SMEM)
    return pl.pallas_call(
        kernel,
        in_specs=[smem] * len(scalars)
        + [pl.BlockSpec(memory_space=pl.ANY)] * len(left)
        + [vmem] * (len(far) + len(near)),
        out_specs=jax.tree.map(lambda _: vmem, shapes),
        out_shape=shapes,
        scratch_shapes=scratch,
        name=name,
    )(*scalars, *left, *far, *(in_vmem(a) for a in near))


def on_device(
    tokens,
    first_gain,
    w_query,
    w_key,
    w_value,
    w_outgate,
    w_input,
    w_forget,
    input_bias,
    forget_bias,
    head_gain,
    w_project,
    cell_state,
    norm_state,
    max_state,
    second_gain,
    routes,
    route_weight,
    expert_gate,
    expert_up,
    expert_down,
):
    blocks = lax.axis_size("ep")
    seq_total, columns = tokens.shape
    seq_local = seq_total // blocks
    value_size = cell_state.shape[3]
    experts = blocks
    slot_count = blocks * CAPACITY

    width = 2 * (w_query.shape[1] + w_value.shape[1])
    handed = (max_state.T, norm_state, head_gain.reshape(1, -1), routes.T, route_weight.T)
    outgoing, old_max, old_norm, gains, route_rows, weight_rows = kernel_call(
        functools.partial(send_kernel, seq_local=seq_local),
        "send_parts",
        [
            pltpu.VMEM((blocks, PADDED, width), BF16),
            *(pltpu.VMEM(a.shape, a.dtype) for a in handed),
        ],
        (),
        far=(
            tokens,
            first_gain.reshape(1, -1),
            w_query,
            w_key,
            w_value,
            w_outgate,
            w_input.T,
            w_forget.T,
            *handed,
        ),
    )
    incoming = exchanged(outgoing, "ep")

    key_size = cell_state.shape[2]
    mixed, *updates = kernel_call(
        functools.partial(receive_kernel, columns=columns),
        "cell_step",
        [
            pltpu.VMEM((blocks, PADDED, value_size), BF16),
            pltpu.VMEM((seq_local, 1), F32),
            pltpu.VMEM((seq_local, key_size), F32),
            pltpu.VMEM((seq_local, value_size), F32),
            pltpu.VMEM((seq_local, key_size), F32),
            pltpu.VMEM((seq_local, 1), F32),
        ],
        (incoming, old_norm, old_max, gains),
        scalars=(input_bias, forget_bias),
        left=(cell_state,),
        scratch=(pltpu.VMEM(cell_state.shape, F32), pltpu.SemaphoreType.DMA),
    )

    part_shape = pltpu.VMEM((seq_total, columns), BF16)
    chip_shape = pltpu.VMEM((lax.axis_size("tp") // 2, seq_total, columns), BF16)
    head_terms = kernel_call(
        functools.partial(project_kernel, seq_local=seq_local),
        "project_heads",
        part_shape,
        (exchanged(mixed, "ep"), w_project),
    )
    chip_terms = kernel_call(
        pair_kernel, "chip_heads", chip_shape, (head_terms, from_other_core(head_terms))
    )
    stream, outbound, table = kernel_call(
        functools.partial(stream_kernel, seq_local=seq_local),
        "stream_rows",
        [
            pltpu.VMEM(tokens.shape, BF16),
            pltpu.VMEM((experts, slot_count, columns), BF16),
            pltpu.VMEM((2 * seq_total, experts * slot_count), BF16),
        ],
        (swapped(chip_terms, chips_of_cores("tp")), tokens, route_rows, weight_rows),
    )

    slot_out = kernel_call(
        expert_kernel,
        "expert",
        pltpu.VMEM((blocks, slot_count, columns), BF16),
        (
            exchanged(outbound, "ep"),
            second_gain.reshape(1, -1),
            expert_gate,
        ),
        left=(expert_up, expert_down),
        scratch=(
            pltpu.VMEM(expert_up.shape, BF16),
            pltpu.VMEM(expert_down.shape, BF16),
            pltpu.SemaphoreType.DMA((2,)),
        ),
    )
    moe_terms = kernel_call(
        combine_kernel, "combine", part_shape, (table, exchanged(slot_out, "ep"))
    )
    moe_terms = kernel_call(
        pair_kernel, "chip_moe", chip_shape, (moe_terms, from_other_core(moe_terms))
    )
    moe_terms, *updates = lax.optimization_barrier((moe_terms, *updates))
    keep_old, admit_key, value, new_norm, new_max = updates
    new_cell = (
        keep_old[:, :, None] * cell_state[:, 0] + admit_key[:, :, None] * value[:, None, :]
    )
    moe_out = jnp.sum(swapped(moe_terms, chips_of_cores("tp")).astype(F32), axis=0)
    layer_out = (stream.astype(F32) + moe_out).astype(BF16)
    return (layer_out, new_cell[:, None], new_norm[:, None], new_max)


def solution(mesh):
    placed = (
        P("grp", "ep"),
        P(),
        P("ep", "tp"),
        P("ep", "tp"),
        P("ep", "tp"),
        P("ep", "tp"),
        P(),
        P(),
        P(),
        P(),
        P(),
        P("tp", "ep"),
        P(("grp", "ep"), "tp", None, None),
        P(("grp", "ep"), "tp", None),
        P(("grp", "ep"), "tp"),
        P(),
        P("grp", None),
        P("grp", None),
        P("ep", None, "tp"),
        P("ep", None, "tp"),
        P("ep", "tp", None),
    )
    return jax.shard_map(
        on_device,
        mesh=mesh,
        in_specs=placed,
        out_specs=(
            P("grp", "ep"),
            P(("grp", "ep"), "tp", None, None),
            P(("grp", "ep"), "tp", None),
            P(("grp", "ep"), "tp"),
        ),
        check_vma=False,
    )
```

```python
import functools

import jax
import jax.numpy as jnp
from jax import lax
from jax.experimental import pallas as pl
from jax.experimental.pallas import tpu as pltpu
from jax.sharding import PartitionSpec as P

NORM_EPS = 1e-05
HEAD_EPS = 1e-06
CAPACITY = 2
LANES = 128
PADDED = 8
GATE_SUMS = 16
F32 = jnp.float32
BF16 = jnp.bfloat16


def exchanged(blocks, axis):
    return lax.all_to_all(blocks, axis, split_axis=0, concat_axis=0, tiled=True)


def from_other_core(array):
    size = lax.axis_size("tp")
    return lax.ppermute(array, "tp", [(i, i ^ 1) for i in range(size)])


def chips_of_cores(axis):
    size = lax.axis_size(axis)
    return [list(range(core, size, 2)) for core in range(2)]


def swapped(blocks, groups):
    return lax.all_to_all(
        blocks, "tp", split_axis=0, concat_axis=0, tiled=True, axis_index_groups=groups
    )


def rounded_pieces(values, count):
    pieces = []
    for _ in range(count):
        head = values.astype(BF16).astype(F32)
        pieces.append(head)
        values = values - head
    return pieces


def dot(a, b):
    return jnp.dot(a, b, preferred_element_type=F32)


def lane_sums(values, count):
    ones = jnp.ones((values.shape[1], LANES), BF16)
    return sum(dot(piece.astype(BF16), ones) for piece in rounded_pieces(values, count))


def grid_index(shape):
    return lax.broadcasted_iota(jnp.int32, shape, 0), lax.broadcasted_iota(jnp.int32, shape, 1)


def one_hot(condition):
    return jnp.where(condition, 1.0, 0.0).astype(BF16)


def send_kernel(cell_hbm, tok_ref, gain_ref, wq, wk, wv, wo, wi, wf, *rest, seq_local):
    *rest, cell_ref, arrived = rest
    fetch = pltpu.make_async_copy(cell_hbm, cell_ref, arrived)
    fetch.start()
    handed = len(rest) // 2
    out_ref = rest[handed]
    for kept, copy in zip(rest[:handed], rest[handed + 1 :]):
        copy[...] = kept[...]
    head = lax.axis_index("tp")
    seq_total, columns = tok_ref.shape
    ours = pl.ds(pl.multiple_of(lax.axis_index("ep") * columns, LANES), columns)
    blocks = seq_total // seq_local
    count = blocks * PADDED
    row, col = grid_index((count, seq_total))
    spread_rows = one_hot(
        ((row & (PADDED - 1)) < seq_local)
        & (col == (row >> 3) * seq_local + (row & (PADDED - 1)))
    )
    slot = lax.broadcasted_iota(jnp.int32, (count, columns), 0) & (PADDED - 1)
    values = dot(spread_rows, tok_ref[...])
    values = jnp.where(slot == seq_local, 1.0, values)
    own = slot < seq_local
    block_mean = jnp.where(own, lane_sums(values, 1) * (1.0 / columns), 0.0)
    offsets = values - block_mean
    moment = jnp.where(own, lane_sums(offsets * offsets, 2), 0.0)
    gain_row = gain_ref[:, ours]
    down, across = grid_index((columns, columns))
    gain_col = lane_sums(jnp.where(down == across, gain_row, 0.0), 3)
    exact = jnp.concatenate([values.astype(BF16)] * 2, axis=1)
    parts = []
    for ref in (wq, wk, wv, wo):
        spread_gain = jnp.concatenate([gain_col] * (ref.shape[1] // LANES), axis=1)
        pieces = rounded_pieces(ref[...].astype(F32) * spread_gain, 2)
        parts.append(dot(exact, jnp.concatenate([p.astype(BF16) for p in pieces], axis=0)))
    product = jnp.concatenate(parts, axis=1)
    tiles = product.reshape(blocks, PADDED, product.shape[1])
    sums = tiles[:, seq_local : seq_local + 1, :]
    wide_mean = jnp.concatenate([block_mean] * (product.shape[1] // LANES), axis=1)
    centred = tiles - wide_mean.reshape(tiles.shape) * sums

    pick, _ = grid_index((wi.shape[0], columns))

    def gate_part(ref):
        chosen = jnp.sum(jnp.where(pick == head, ref[:, ours].astype(F32), 0.0), axis=0, keepdims=True)
        return lane_sums(offsets * (chosen * gain_row), 3)

    gates = [*rounded_pieces(gate_part(wi), 2), *rounded_pieces(gate_part(wf), 2)]
    lane = lax.broadcasted_iota(jnp.int32, (count, LANES), 1)
    start = jnp.where(slot == seq_local, GATE_SUMS, 0)
    table = jnp.zeros((count, LANES), F32)
    for k, piece in enumerate(gates):
        table = jnp.where(lane == start + k, piece, table)
    table = jnp.where(slot == PADDED - 1, 0.0, table)
    for k, piece in enumerate([*rounded_pieces(block_mean, 3), *rounded_pieces(moment, 2)]):
        table = jnp.where((lane == 4 + k) & own, piece, table)
    exact_table = table.astype(BF16)
    down, across = grid_index((count, count))
    same = (down >> 3) == (across >> 3)
    last = (down & (PADDED - 1)) == PADDED - 1
    inner = across & (PADDED - 1)
    moves = [
        one_hot(same & last & ((inner == r) | (inner == seq_local))) for r in range(seq_local)
    ]
    laid = dot(jnp.concatenate(moves, axis=0), exact_table)
    side = jnp.concatenate(
        [laid[r * count : (r + 1) * count] for r in range(seq_local)], axis=1
    ).reshape(tiles.shape)
    out_ref[...] = (centred + side).astype(BF16)
    fetch.wait()


def receive_kernel(
    in_bias, for_bias, got_ref, cell_ref, norm_ref, max_ref, gain_ref,
    mixed_ref, keep_ref, admit_ref, value_ref, norm_out, max_out, *, columns
):
    head = lax.axis_index("tp")
    blocks, padded, width = got_ref.shape
    seq_local, _, key_size, value_size = cell_ref.shape
    count = blocks * padded
    got = got_ref[...].astype(F32)
    flat = got.reshape(count, width).astype(BF16)
    down, across = grid_index((count, count))
    same = (down >> 3) == (across >> 3)
    inner = across & (PADDED - 1)
    outer = down & (PADDED - 1)
    moves = [
        one_hot(same & (outer == r) & (inner == PADDED - 1)) for r in range(seq_local)
    ]
    table = dot(
        jnp.concatenate(moves, axis=1),
        jnp.concatenate([flat[:, r * LANES : (r + 1) * LANES] for r in range(seq_local)], axis=0),
    )
    sums = got[:, seq_local : seq_local + 1, :]
    lane, _ = grid_index((LANES, LANES))
    spans = ((4, 3), (7, 2), (0, 2), (GATE_SUMS, 2), (2, 2), (GATE_SUMS + 2, 2))
    chosen = [one_hot((lane >= first) & (lane < first + number)) for first, number in spans]
    gathered = dot(table.astype(BF16), jnp.concatenate(chosen, axis=1))

    def term(k):
        return gathered[:, k * LANES : (k + 1) * LANES].reshape(blocks, padded, LANES)

    means = term(0)
    row_mean = jnp.sum(means, axis=0, keepdims=True) * (1.0 / blocks)
    shifts = means - row_mean
    spread = jnp.sum(term(1) + columns * shifts * shifts, axis=0) * (1.0 / (blocks * columns))
    inv_scale = lax.rsqrt(spread + NORM_EPS)
    parts = width // LANES
    wide_shifts = jnp.concatenate([shifts] * parts, axis=2)
    projected = jnp.concatenate([inv_scale] * parts, axis=1) * jnp.sum(
        got + wide_shifts * sums, axis=0
    )

    def rounded(a, b):
        return projected[:, a:b].astype(BF16).astype(F32)

    query = rounded(0, key_size) * key_size**-0.5
    key = rounded(key_size, 2 * key_size)
    value = rounded(2 * key_size, 2 * key_size + value_size)
    outgate = rounded(2 * key_size + value_size, width)
    input_pre = (
        inv_scale * jnp.sum(term(2) + shifts * term(3), axis=0) + in_bias[head]
    )
    forget_pre = (
        inv_scale * jnp.sum(term(4) + shifts * term(5), axis=0)
        + for_bias[head]
    )
    down, across = grid_index((padded, seq_local))
    old_max = jnp.sum(jnp.where(down == across, max_ref[...], 0.0), axis=1, keepdims=True)
    log_forget = jnp.minimum(forget_pre, 0.0) - jnp.log1p(jnp.exp(-jnp.abs(forget_pre)))
    carried = log_forget + old_max
    new_max = jnp.maximum(carried, input_pre)
    keep_old = jnp.exp(carried - new_max)
    admit_key = jnp.exp(input_pre - new_max) * key
    max_out[...] = new_max[:seq_local, :1]
    keep_ref[...] = keep_old[:seq_local, :1]
    admit_ref[...] = admit_key[:seq_local]
    value_ref[...] = value[:seq_local]
    query_cols = query.T
    rows = lax.broadcasted_iota(jnp.int32, (padded, value_size), 0)
    against_cell = jnp.zeros((padded, value_size), F32)
    for s in range(seq_local):
        norm_out[s : s + 1] = keep_old[s : s + 1] * norm_ref[s] + admit_key[s : s + 1]
        read = jnp.sum(query_cols[:, s : s + 1] * cell_ref[s, 0], axis=0, keepdims=True)
        against_cell = jnp.where(rows == s, read, against_cell)
    scores = jnp.sum(query * admit_key, axis=1, keepdims=True)
    wide_keep = jnp.concatenate([keep_old] * (value_size // LANES), axis=1)
    readout = jnp.where(rows < seq_local, wide_keep * against_cell + scores * value, 0.0)
    outgate = jnp.where(rows < seq_local, outgate, 0.0)
    head_mean = jnp.mean(readout, axis=1, keepdims=True)
    around = readout - head_mean
    head_var = jnp.mean(around * around, axis=1, keepdims=True)
    gain = gain_ref[:, pl.ds(pl.multiple_of(head * value_size, LANES), value_size)]
    opened = 1.0 / (1.0 + jnp.exp(-outgate))
    mixed = around * lax.rsqrt(head_var + HEAD_EPS) * gain * opened
    mixed_ref[...] = jnp.broadcast_to(mixed[None], (blocks, padded, value_size)).astype(BF16)


def project_kernel(got_ref, weight_ref, out_ref, *, seq_local):
    blocks, padded, width = got_ref.shape
    seq_total = out_ref.shape[0]
    rows = got_ref[...].astype(F32).reshape(blocks * padded, width).astype(BF16)
    terms = dot(rows, weight_ref[...]).astype(BF16)
    row, col = grid_index((seq_total, blocks * padded))
    inner = col & (PADDED - 1)
    packed = dot(one_hot((inner < seq_local) & (row == (col >> 3) * seq_local + inner)), terms)
    out_ref[...] = packed.astype(BF16)


def pair_kernel(own_ref, other_ref, out_ref):
    added = (own_ref[...].astype(F32) + other_ref[...].astype(F32)).astype(BF16)
    out_ref[...] = jnp.broadcast_to(added[None], out_ref.shape)


def column_of(row):
    down, across = grid_index((row.shape[1], row.shape[1]))
    return jnp.sum(jnp.where(down == across, row, 0.0), axis=1, keepdims=True)


def stream_kernel(
    got_ref, tok_ref, route_ref, weight_ref, stream_ref, out_ref, table_ref, *, seq_local
):
    mixer_out = jnp.sum(got_ref[...].astype(F32), axis=0)
    stream = (tok_ref[...].astype(F32) + mixer_out).astype(BF16)
    stream_ref[...] = stream
    top, seq_total = route_ref.shape
    experts, slots, _ = out_ref.shape
    names = [route_ref[k : k + 1].astype(F32) for k in range(top)]
    down, across = grid_index((seq_total, seq_total))
    block_down = jnp.floor((down.astype(F32) + 0.5) * (1.0 / seq_local))
    block_across = jnp.floor((across.astype(F32) + 0.5) * (1.0 / seq_local))
    earlier = (block_down == block_across) & (across < down)
    place = lax.broadcasted_iota(jnp.int32, (seq_total, experts * slots), 1).astype(F32)
    picked = jnp.zeros(place.shape, F32)
    weights = jnp.zeros(place.shape, F32)
    for k in range(top):
        name = column_of(names[k])
        same = sum(jnp.where(earlier & (other == name), 1.0, 0.0) for other in names)
        slot = name * slots + block_down[:, :1] * CAPACITY + jnp.sum(same, axis=1, keepdims=True)
        here = place == slot
        picked = jnp.where(here, 1.0, picked)
        weights = jnp.where(here, column_of(weight_ref[k : k + 1]), weights)
    table = [piece.astype(BF16) for piece in rounded_pieces(weights, 2)]
    table_ref[...] = jnp.concatenate(table, axis=0)
    chosen = lax.dot_general(
        picked.astype(BF16), stream, (((0,), (0,)), ((), ())), preferred_element_type=F32
    )
    out_ref[...] = chosen.astype(BF16).reshape(out_ref.shape)


def expert_kernel(
    down_hbm, got_ref, gain_ref, gate_ref, up_ref, out_ref, down_ref, arrived
):
    fetch = pltpu.make_async_copy(down_hbm, down_ref, arrived)
    fetch.start()
    blocks, _, columns = got_ref.shape
    values = jnp.concatenate([got_ref[e].astype(F32) for e in range(blocks)], axis=1)
    row_mean = jnp.mean(values, axis=1, keepdims=True)
    spread = jnp.mean(values * values, axis=1, keepdims=True) - row_mean * row_mean
    normed = ((values - row_mean) * lax.rsqrt(spread + NORM_EPS) * gain_ref[...]).astype(BF16)
    gate = dot(normed, gate_ref[0])
    active = (gate / (1.0 + jnp.exp(-gate)) * dot(normed, up_ref[0])).astype(BF16)
    fetch.wait()
    result = dot(active, down_ref[0]).astype(BF16)
    for e in range(blocks):
        out_ref[e] = result[:, e * columns : (e + 1) * columns]


def combine_kernel(table_ref, back_ref, out_ref):
    seq_total = out_ref.shape[0]
    experts, slots, columns = back_ref.shape
    both = dot(table_ref[...], back_ref[...].reshape(experts * slots, columns))
    out_ref[...] = (both[:seq_total] + both[seq_total:]).astype(BF16)


def in_vmem(array):
    return pltpu.with_memory_space_constraint(array, pltpu.VMEM)


def kernel_call(kernel, name, shapes, near, scalars=(), far=(), left=(), scratch=()):
    vmem = pl.BlockSpec(memory_space=pltpu.VMEM)
    smem = pl.BlockSpec(memory_space=pltpu.SMEM)
    return pl.pallas_call(
        kernel,
        in_specs=[smem] * len(scalars)
        + [pl.BlockSpec(memory_space=pl.ANY)] * len(left)
        + [vmem] * (len(far) + len(near)),
        out_specs=jax.tree.map(lambda _: vmem, shapes),
        out_shape=shapes,
        scratch_shapes=scratch,
        name=name,
    )(*scalars, *left, *far, *(in_vmem(a) for a in near))


def on_device(
    tokens,
    first_gain,
    w_query,
    w_key,
    w_value,
    w_outgate,
    w_input,
    w_forget,
    input_bias,
    forget_bias,
    head_gain,
    w_project,
    cell_state,
    norm_state,
    max_state,
    second_gain,
    routes,
    route_weight,
    expert_gate,
    expert_up,
    expert_down,
):
    blocks = lax.axis_size("ep")
    seq_total, columns = tokens.shape
    seq_local = seq_total // blocks
    value_size = cell_state.shape[3]
    experts = blocks
    slot_count = blocks * CAPACITY

    width = 2 * (w_query.shape[1] + w_value.shape[1])
    handed = (max_state.T, norm_state, head_gain.reshape(1, -1), routes.T, route_weight.T)
    outgoing, old_max, old_norm, gains, route_rows, weight_rows, old_cell = kernel_call(
        functools.partial(send_kernel, seq_local=seq_local),
        "send_parts",
        [
            pltpu.VMEM((blocks, PADDED, width), BF16),
            *(pltpu.VMEM(a.shape, a.dtype) for a in (*handed, cell_state)),
        ],
        (),
        far=(
            tokens,
            first_gain.reshape(1, -1),
            w_query,
            w_key,
            w_value,
            w_outgate,
            w_input.T,
            w_forget.T,
            *handed,
        ),
        left=(cell_state,),
        scratch=(pltpu.SemaphoreType.DMA,),
    )
    incoming = exchanged(outgoing, "ep")

    key_size = cell_state.shape[2]
    mixed, *updates = kernel_call(
        functools.partial(receive_kernel, columns=columns),
        "cell_step",
        [
            pltpu.VMEM((blocks, PADDED, value_size), BF16),
            pltpu.VMEM((seq_local, 1), F32),
            pltpu.VMEM((seq_local, key_size), F32),
            pltpu.VMEM((seq_local, value_size), F32),
            pltpu.VMEM((seq_local, key_size), F32),
            pltpu.VMEM((seq_local, 1), F32),
        ],
        (incoming, old_cell, old_norm, old_max, gains),
        scalars=(input_bias, forget_bias),
    )

    part_shape = pltpu.VMEM((seq_total, columns), BF16)
    chip_shape = pltpu.VMEM((lax.axis_size("tp") // 2, seq_total, columns), BF16)
    head_terms = kernel_call(
        functools.partial(project_kernel, seq_local=seq_local),
        "project_heads",
        part_shape,
        (exchanged(mixed, "ep"), w_project),
    )
    chip_terms = kernel_call(
        pair_kernel, "chip_heads", chip_shape, (head_terms, from_other_core(head_terms))
    )
    stream, outbound, table = kernel_call(
        functools.partial(stream_kernel, seq_local=seq_local),
        "stream_rows",
        [
            pltpu.VMEM(tokens.shape, BF16),
            pltpu.VMEM((experts, slot_count, columns), BF16),
            pltpu.VMEM((2 * seq_total, experts * slot_count), BF16),
        ],
        (swapped(chip_terms, chips_of_cores("tp")), tokens, route_rows, weight_rows),
    )

    slot_out = kernel_call(
        expert_kernel,
        "expert",
        pltpu.VMEM((blocks, slot_count, columns), BF16),
        (
            exchanged(outbound, "ep"),
            second_gain.reshape(1, -1),
            expert_gate,
            expert_up,
        ),
        left=(expert_down,),
        scratch=(pltpu.VMEM(expert_down.shape, BF16), pltpu.SemaphoreType.DMA),
    )
    moe_terms = kernel_call(
        combine_kernel, "combine", part_shape, (table, exchanged(slot_out, "ep"))
    )
    moe_terms = kernel_call(
        pair_kernel, "chip_moe", chip_shape, (moe_terms, from_other_core(moe_terms))
    )
    moe_terms, *updates = lax.optimization_barrier((moe_terms, *updates))
    keep_old, admit_key, value, new_norm, new_max = updates
    new_cell = (
        keep_old[:, :, None] * cell_state[:, 0] + admit_key[:, :, None] * value[:, None, :]
    )
    moe_out = jnp.sum(swapped(moe_terms, chips_of_cores("tp")).astype(F32), axis=0)
    layer_out = (stream.astype(F32) + moe_out).astype(BF16)
    return (layer_out, new_cell[:, None], new_norm[:, None], new_max)


def solution(mesh):
    placed = (
        P("grp", "ep"),
        P(),
        P("ep", "tp"),
        P("ep", "tp"),
        P("ep", "tp"),
        P("ep", "tp"),
        P(),
        P(),
        P(),
        P(),
        P(),
        P("tp", "ep"),
        P(("grp", "ep"), "tp", None, None),
        P(("grp", "ep"), "tp", None),
        P(("grp", "ep"), "tp"),
        P(),
        P("grp", None),
        P("grp", None),
        P("ep", None, "tp"),
        P("ep", None, "tp"),
        P("ep", "tp", None),
    )
    return jax.shard_map(
        on_device,
        mesh=mesh,
        in_specs=placed,
        out_specs=(
            P("grp", "ep"),
            P(("grp", "ep"), "tp", None, None),
            P(("grp", "ep"), "tp", None),
            P(("grp", "ep"), "tp"),
        ),
        check_vma=False,
    )
```

```python
import functools

import jax
import jax.numpy as jnp
from jax import lax
from jax.experimental import pallas as pl
from jax.experimental.pallas import tpu as pltpu
from jax.sharding import PartitionSpec as P

NORM_EPS = 1e-05
HEAD_EPS = 1e-06
CAPACITY = 2
LANES = 128
PADDED = 8
GATE_SUMS = 16
F32 = jnp.float32
BF16 = jnp.bfloat16


def exchanged(blocks, axis):
    return lax.all_to_all(blocks, axis, split_axis=0, concat_axis=0, tiled=True)


def from_other_core(array):
    size = lax.axis_size("tp")
    return lax.ppermute(array, "tp", [(i, i ^ 1) for i in range(size)])


def chips_of_cores(axis):
    size = lax.axis_size(axis)
    return [list(range(core, size, 2)) for core in range(2)]


def swapped(blocks, groups):
    return lax.all_to_all(
        blocks, "tp", split_axis=0, concat_axis=0, tiled=True, axis_index_groups=groups
    )


def rounded_pieces(values, count):
    pieces = []
    for _ in range(count):
        head = values.astype(BF16).astype(F32)
        pieces.append(head)
        values = values - head
    return pieces


def dot(a, b):
    return jnp.dot(a, b, preferred_element_type=F32)


def lane_sums(values, count):
    ones = jnp.ones((values.shape[1], LANES), BF16)
    return sum(dot(piece.astype(BF16), ones) for piece in rounded_pieces(values, count))


def grid_index(shape):
    return lax.broadcasted_iota(jnp.int32, shape, 0), lax.broadcasted_iota(jnp.int32, shape, 1)


def one_hot(condition):
    return jnp.where(condition, 1.0, 0.0).astype(BF16)


def from_everyone(array, axis):
    peers = lax.axis_size(axis)
    return lax.all_to_all(
        jnp.broadcast_to(array[None], (peers, *array.shape)), axis, 0, 0, tiled=True
    )


def taken_together(array, axis):
    everything = from_everyone(array, axis)
    return jnp.sum(everything, axis=0)


def in_one(arrays, axis):
    ends = [0]
    for a in arrays:
        ends.append(ends[-1] + a.size)
    subtotal = taken_together(jnp.concatenate([a.ravel() for a in arrays]), axis)
    return tuple((subtotal[b:e].reshape(a.shape) for a, b, e in zip(arrays, ends, ends[1:])))


def cut_along(array, dim, peers):
    lengths = array.shape
    blocks = array.reshape(*lengths[:dim], peers, lengths[dim] // peers, *lengths[dim + 1 :])
    return jnp.moveaxis(blocks, dim, 0)


def summed_on_arrival_2(array, axis, dim):
    blocks = cut_along(array, dim, lax.axis_size(axis))
    arrived = lax.all_to_all(blocks, axis, split_axis=0, concat_axis=0, tiled=True)
    return arrived.sum(axis=0)


def side_by_side(arrays, axis, dim, along):
    ends, at = ([], 0)
    for a in arrays[:-1]:
        at += a.shape[along]
        ends.append(at)
    both = jnp.concatenate(arrays, axis=along)
    return tuple(jnp.split(summed_on_arrival_2(both, axis, dim), ends, axis=along))


def row_norm(stream_rows, gain_whole):
    col_count = stream_rows.shape[1]
    gain_cols = lax.dynamic_slice_in_dim(gain_whole, lax.axis_index("ep") * col_count, col_count, 0)
    values = stream_rows.astype(jnp.float32)
    totals, squares = in_one((jnp.sum(values, axis=1), jnp.sum(values * values, axis=1)), "ep")
    features = col_count * lax.axis_size("ep")
    row_mean = totals / features
    spread = squares / features - row_mean * row_mean
    inv_scale = lax.rsqrt(spread + NORM_EPS)
    return ((values - row_mean[:, None]) * inv_scale[:, None] * gain_cols).astype(jnp.bfloat16)


def project_kernel(got_ref, weight_ref, out_ref, *, seq_local):
    blocks, padded, width = got_ref.shape
    seq_total = out_ref.shape[0]
    rows = got_ref[...].astype(F32).reshape(blocks * padded, width).astype(BF16)
    terms = dot(rows, weight_ref[...]).astype(BF16)
    row, col = grid_index((seq_total, blocks * padded))
    inner = col & (PADDED - 1)
    packed = dot(one_hot((inner < seq_local) & (row == (col >> 3) * seq_local + inner)), terms)
    out_ref[...] = packed.astype(BF16)


def pair_kernel(own_ref, other_ref, out_ref):
    added = (own_ref[...].astype(F32) + other_ref[...].astype(F32)).astype(BF16)
    out_ref[...] = jnp.broadcast_to(added[None], out_ref.shape)


def column_of(row):
    down, across = grid_index((row.shape[1], row.shape[1]))
    return jnp.sum(jnp.where(down == across, row, 0.0), axis=1, keepdims=True)


def stream_kernel(
    got_ref, tok_ref, route_ref, weight_ref, stream_ref, out_ref, table_ref, *, seq_local
):
    mixer_out = jnp.sum(got_ref[...].astype(F32), axis=0)
    stream = (tok_ref[...].astype(F32) + mixer_out).astype(BF16)
    stream_ref[...] = stream
    top, seq_total = route_ref.shape
    experts, slots, _ = out_ref.shape
    names = [route_ref[k : k + 1].astype(F32) for k in range(top)]
    down, across = grid_index((seq_total, seq_total))
    block_down = jnp.floor((down.astype(F32) + 0.5) * (1.0 / seq_local))
    block_across = jnp.floor((across.astype(F32) + 0.5) * (1.0 / seq_local))
    earlier = (block_down == block_across) & (across < down)
    place = lax.broadcasted_iota(jnp.int32, (seq_total, experts * slots), 1).astype(F32)
    picked = jnp.zeros(place.shape, F32)
    weights = jnp.zeros(place.shape, F32)
    for k in range(top):
        name = column_of(names[k])
        same = sum(jnp.where(earlier & (other == name), 1.0, 0.0) for other in names)
        slot = name * slots + block_down[:, :1] * CAPACITY + jnp.sum(same, axis=1, keepdims=True)
        here = place == slot
        picked = jnp.where(here, 1.0, picked)
        weights = jnp.where(here, column_of(weight_ref[k : k + 1]), weights)
    table = [piece.astype(BF16) for piece in rounded_pieces(weights, 2)]
    table_ref[...] = jnp.concatenate(table, axis=0)
    chosen = lax.dot_general(
        picked.astype(BF16), stream, (((0,), (0,)), ((), ())), preferred_element_type=F32
    )
    out_ref[...] = chosen.astype(BF16).reshape(out_ref.shape)


def expert_kernel(
    up_hbm, down_hbm, got_ref, gain_ref, gate_ref, out_ref, up_ref, down_ref, arrived
):
    fetches = [
        pltpu.make_async_copy(up_hbm, up_ref, arrived.at[0]),
        pltpu.make_async_copy(down_hbm, down_ref, arrived.at[1]),
    ]
    for fetch in fetches:
        fetch.start()
    blocks, _, columns = got_ref.shape
    values = jnp.concatenate([got_ref[e].astype(F32) for e in range(blocks)], axis=1)
    row_mean = jnp.mean(values, axis=1, keepdims=True)
    spread = jnp.mean(values * values, axis=1, keepdims=True) - row_mean * row_mean
    normed = ((values - row_mean) * lax.rsqrt(spread + NORM_EPS) * gain_ref[...]).astype(BF16)
    gate = dot(normed, gate_ref[0])
    fetches[0].wait()
    active = (gate / (1.0 + jnp.exp(-gate)) * dot(normed, up_ref[0])).astype(BF16)
    fetches[1].wait()
    result = dot(active, down_ref[0]).astype(BF16)
    for e in range(blocks):
        out_ref[e] = result[:, e * columns : (e + 1) * columns]


def combine_kernel(table_ref, back_ref, out_ref):
    seq_total = out_ref.shape[0]
    experts, slots, columns = back_ref.shape
    both = dot(table_ref[...], back_ref[...].reshape(experts * slots, columns))
    out_ref[...] = (both[:seq_total] + both[seq_total:]).astype(BF16)


def in_vmem(array):
    return pltpu.with_memory_space_constraint(array, pltpu.VMEM)


def kernel_call(kernel, name, shapes, near, scalars=(), far=(), left=(), scratch=()):
    vmem = pl.BlockSpec(memory_space=pltpu.VMEM)
    smem = pl.BlockSpec(memory_space=pltpu.SMEM)
    return pl.pallas_call(
        kernel,
        in_specs=[smem] * len(scalars)
        + [pl.BlockSpec(memory_space=pl.ANY)] * len(left)
        + [vmem] * (len(far) + len(near)),
        out_specs=jax.tree.map(lambda _: vmem, shapes),
        out_shape=shapes,
        scratch_shapes=scratch,
        name=name,
    )(*scalars, *left, *far, *(in_vmem(a) for a in near))


def on_device(
    tokens,
    first_gain,
    w_query,
    w_key,
    w_value,
    w_outgate,
    w_input,
    w_forget,
    input_bias,
    forget_bias,
    head_gain,
    w_project,
    cell_state,
    norm_state,
    max_state,
    second_gain,
    routes,
    route_weight,
    expert_gate,
    expert_up,
    expert_down,
):
    blocks = lax.axis_size("ep")
    seq_total, columns = tokens.shape
    seq_local = seq_total // blocks
    heads_local = cell_state.shape[1]
    key_size = cell_state.shape[2]
    value_size = cell_state.shape[3]
    col_start = lax.axis_index("ep") * columns
    head_start = lax.axis_index("tp") * heads_local
    normed = row_norm(tokens, first_gain)
    input_cols = lax.dynamic_slice(w_input, (col_start, head_start), (columns, heads_local))
    forget_cols = lax.dynamic_slice(w_forget, (col_start, head_start), (columns, heads_local))

    def project_part(weight):
        return jnp.dot(normed, weight, preferred_element_type=jnp.float32)

    summed = side_by_side(
        (
            project_part(w_query),
            project_part(w_key),
            project_part(w_value),
            project_part(w_outgate),
            project_part(input_cols),
            project_part(forget_cols),
        ),
        "ep",
        0,
        1,
    )
    queries = summed[0].astype(jnp.bfloat16).reshape(seq_local, heads_local, key_size)
    key_rows = summed[1].astype(jnp.bfloat16).reshape(seq_local, heads_local, key_size)
    value_rows = summed[2].astype(jnp.bfloat16).reshape(seq_local, heads_local, value_size)
    outgate = summed[3].astype(jnp.bfloat16)
    input_pre = summed[4] + lax.dynamic_slice_in_dim(input_bias, head_start, heads_local, 0)
    forget_pre = summed[5] + lax.dynamic_slice_in_dim(forget_bias, head_start, heads_local, 0)
    carried = jax.nn.log_sigmoid(forget_pre) + max_state
    new_max = jnp.maximum(carried, input_pre)
    keep_old = jnp.exp(carried - new_max)
    admit_new = jnp.exp(input_pre - new_max)
    key_float = key_rows.astype(jnp.float32)
    value_float = value_rows.astype(jnp.float32)
    new_cell = (
        keep_old[:, :, None, None] * cell_state
        + admit_new[:, :, None, None] * key_float[:, :, :, None] * value_float[:, :, None, :]
    )
    new_norm = keep_old[:, :, None] * norm_state + admit_new[:, :, None] * key_float
    query_float = queries.astype(jnp.float32) * key_size ** (-0.5)
    readout = jnp.einsum("shk,shkv->shv", query_float, new_cell, precision=lax.Precision.HIGHEST)
    head_mean = jnp.mean(readout, axis=2, keepdims=True)
    centred = readout - head_mean
    head_var = jnp.mean(centred * centred, axis=2, keepdims=True)
    gains_here = lax.dynamic_slice_in_dim(
        head_gain, head_start * value_size, heads_local * value_size, 0
    )
    mixed_heads = (
        (centred * lax.rsqrt(head_var + HEAD_EPS)).reshape(seq_local, heads_local * value_size)
        * gains_here
        * jax.nn.sigmoid(outgate.astype(jnp.float32))
    ).astype(jnp.bfloat16)
    experts = blocks
    slot_count = blocks * CAPACITY
    padded = jnp.pad(mixed_heads, ((0, PADDED - seq_local), (0, 0)))
    mixed = jnp.broadcast_to(padded[None], (blocks, PADDED, value_size))
    part_shape = pltpu.VMEM((seq_total, columns), BF16)
    chip_shape = pltpu.VMEM((lax.axis_size("tp") // 2, seq_total, columns), BF16)
    head_terms = kernel_call(
        functools.partial(project_kernel, seq_local=seq_local),
        "project_heads",
        part_shape,
        (exchanged(mixed, "ep"), w_project),
    )
    chip_terms = kernel_call(
        pair_kernel, "chip_heads", chip_shape, (head_terms, from_other_core(head_terms))
    )
    stream, outbound, table = kernel_call(
        functools.partial(stream_kernel, seq_local=seq_local),
        "stream_rows",
        [
            pltpu.VMEM(tokens.shape, BF16),
            pltpu.VMEM((experts, slot_count, columns), BF16),
            pltpu.VMEM((2 * seq_total, experts * slot_count), BF16),
        ],
        (swapped(chip_terms, chips_of_cores("tp")), tokens, routes.T, route_weight.T),
    )

    slot_out = kernel_call(
        expert_kernel,
        "expert",
        pltpu.VMEM((blocks, slot_count, columns), BF16),
        (
            exchanged(outbound, "ep"),
            second_gain.reshape(1, -1),
            expert_gate,
        ),
        left=(expert_up, expert_down),
        scratch=(
            pltpu.VMEM(expert_up.shape, BF16),
            pltpu.VMEM(expert_down.shape, BF16),
            pltpu.SemaphoreType.DMA((2,)),
        ),
    )
    moe_terms = kernel_call(
        combine_kernel, "combine", part_shape, (table, exchanged(slot_out, "ep"))
    )
    moe_terms = kernel_call(
        pair_kernel, "chip_moe", chip_shape, (moe_terms, from_other_core(moe_terms))
    )
    moe_out = jnp.sum(swapped(moe_terms, chips_of_cores("tp")).astype(F32), axis=0)
    layer_out = (stream.astype(F32) + moe_out).astype(BF16)
    return (layer_out, new_cell, new_norm, new_max)


def solution(mesh):
    placed = (
        P("grp", "ep"),
        P(),
        P("ep", "tp"),
        P("ep", "tp"),
        P("ep", "tp"),
        P("ep", "tp"),
        P(),
        P(),
        P(),
        P(),
        P(),
        P("tp", "ep"),
        P(("grp", "ep"), "tp", None, None),
        P(("grp", "ep"), "tp", None),
        P(("grp", "ep"), "tp"),
        P(),
        P("grp", None),
        P("grp", None),
        P("ep", None, "tp"),
        P("ep", None, "tp"),
        P("ep", "tp", None),
    )
    return jax.shard_map(
        on_device,
        mesh=mesh,
        in_specs=placed,
        out_specs=(
            P("grp", "ep"),
            P(("grp", "ep"), "tp", None, None),
            P(("grp", "ep"), "tp", None),
            P(("grp", "ep"), "tp"),
        ),
        check_vma=False,
    )
```
